256 devices in a mesh: dp: 4 (over y), kv: 32 (over z, x), tp: 2 (over core).
Axes of the slice: x: 4, y: 4, z: 8, core: 2. Of those that a mesh axis runs over, the one named last changes fastest.
Arguments:
- tokens: bfloat16 [256, 4096], P('dp', ('kv', 'tp')), as said below
- query_weight: bfloat16 [4096, 16, 128], P(None, 'tp', 'kv'), may hold values from -0.09375 to 0.09375
- key_weight: bfloat16 [4096, 16, 128], P(None, 'tp', 'kv'), may hold values from -0.09375 to 0.09375
- value_weight: bfloat16 [4096, 16, 256], P(None, 'tp', 'kv'), may hold values from -0.09375 to 0.09375
- gate_weight: bfloat16 [4096, 16, 256], P(None, 'tp', 'kv'), may hold values from -0.09375 to 0.09375
- decay_weight: bfloat16 [4096, 16, 128], P(None, 'tp', 'kv'), may hold values from -0.09375 to 0.09375
- decay_bias: float32 [16, 128], P('tp'), may hold values from -8 to 2
- states: float32 [256, 16, 128, 256], P(('dp', 'kv'), 'tp'), may hold values from -4 to 4
- head_gain: float32 [16, 256], P('tp'), may hold values from 0.1 to 1.9
- out_weight: bfloat16 [4096, 4096], P(None, ('kv', 'tp')), as said below
- norm1_gain: float32 [4096], P(('kv', 'tp')), may hold values from 0.1 to 1.9
- norm1_bias: float32 [4096], P(('kv', 'tp')), may hold values from -3 to 3
- up_weight: bfloat16 [4096, 16384], P(None, ('kv', 'tp')), may hold values from -0.09375 to 0.09375
- down_weight: bfloat16 [16384, 4096], P(('kv', 'tp')), as said below
- norm2_gain: float32 [4096], P(('kv', 'tp')), may hold values from 0.1 to 1.9
- norm2_bias: float32 [4096], P(('kv', 'tp')), may hold values from -3 to 3
Outputs:
- layer_out: bfloat16 [256, 4096], P('dp', ('kv', 'tp'))
- new_states: float32 [256, 16, 128, 256], P(('dp', 'kv'), 'tp')
The draws below stay inside these ranges and needn't reach their ends.
Inputs may be any that keep to these rules, and one draw needn't show every extreme that they name: `tokens`: each block of 64 features has its own scale. `out_weight`: entries lie within 13 / sqrt(4096) of zero. `down_weight`: entries lie within 14 / sqrt(16384) of zero.
All inputs are finite; a program needn't handle non-finite values.
Results may differ from the reference program's by a relative error of at most 0.009.
Values may be sent and summed in bfloat16 or wider, within the bound.
A program may use at most 64 MiB of HBM per device.

```python
import jax
import jax.numpy as jnp
from jax import lax

D = 4096
HEADS = 16
KEY_DIM = 128
VALUE_DIM = 256
MIXER_UNITS = 16384
ROWS = 256


def draw_tokens(key, part):
    base_key, scale_key = jax.random.split(key, 2)
    column_scale = jnp.exp(jax.random.uniform(scale_key, (D // 64,), jnp.float32, -1.0, 1.0))
    column_scale = jnp.repeat(column_scale, 64)
    values = jax.random.normal(base_key, (ROWS, D), jnp.float32)
    return (values * column_scale).astype(jnp.bfloat16)


def draw_out_weight(key, part):
    noise_key, left_key, right_key = jax.random.split(jax.random.fold_in(key, 31), 3)
    fan_in = HEADS * VALUE_DIM
    left = jnp.clip(jax.random.normal(left_key, (fan_in, 1), jnp.float32), -3.0, 3.0)
    right = jnp.clip(jax.random.normal(right_key, (1, D), jnp.float32), -3.0, 3.0)
    noise = jnp.clip(jax.random.normal(noise_key, (fan_in, D), jnp.float32), -6.0, 6.0)
    common = 0.8 * left * right
    return ((0.6 * noise + common) * fan_in ** (-0.5)).astype(jnp.bfloat16)


def draw_down_weight(key, part):
    noise_key, offset_key = jax.random.split(jax.random.fold_in(key, 47), 2)
    noise = jnp.clip(jax.random.normal(noise_key, (MIXER_UNITS, D), jnp.float32), -6.0, 6.0)
    offset = jax.random.uniform(offset_key, (1, D), jnp.float32, -5.0, 5.0)
    values = noise * MIXER_UNITS ** (-0.5) + offset / MIXER_UNITS
    return values.astype(jnp.bfloat16)


def block_levels(own_key, dims, shards, low, top_value):
    level, own = 1.0, jax.random.fold_in(own_key, 6)
    for dim, blocks in shards:
        steps = jnp.exp(jax.random.uniform(jax.random.fold_in(own, dim), (blocks,), jnp.float32, low / len(shards), top_value / len(shards)))
        level = level * jnp.repeat(steps, dims[dim] // blocks).reshape([-1 if axis == dim else 1 for axis in range(len(dims))])
    return level


def scatter_about(stream_key, shape, scale, reach, cuts=(), kind=jnp.bfloat16):
    values = scale * jax.random.normal(stream_key, shape, jnp.float32)
    if cuts:
        values = values * block_levels(stream_key, shape, cuts, -0.22, 0.18)
    return jnp.clip(values, -reach, reach).astype(kind)


def setup_inputs(seed: int = 0) -> dict:
    keys = jax.random.split(jax.random.key(seed), 17)
    return {
        "tokens": draw_tokens(jax.random.fold_in(keys[16], 71), 0),
        "query_weight": scatter_about(keys[1], (D, HEADS, KEY_DIM), D ** -0.5, 0.09375, ((1, 2), (2, 32))),
        "key_weight": scatter_about(keys[2], (D, HEADS, KEY_DIM), D ** -0.5, 0.09375, ((1, 2), (2, 32))),
        "value_weight": scatter_about(keys[3], (D, HEADS, VALUE_DIM), D ** -0.5, 0.09375, ((1, 2), (2, 32))),
        "gate_weight": scatter_about(keys[4], (D, HEADS, VALUE_DIM), D ** -0.5, 0.09375, ((1, 2), (2, 32))),
        "decay_weight": scatter_about(keys[5], (D, HEADS, KEY_DIM), D ** -0.5, 0.09375, ((1, 2), (2, 32))),
        "decay_bias": jnp.clip(-8.0 + 10.0 * jax.random.uniform(keys[6], (HEADS, KEY_DIM), jnp.float32) ** block_levels(keys[6], (HEADS, KEY_DIM), ((0, 2),), -0.2, 0.2), -8.0, 2.0),
        "states": scatter_about(keys[7], (ROWS, HEADS, KEY_DIM, VALUE_DIM), 0.5, 4.0, ((0, 128), (1, 2)), jnp.float32),
        "head_gain": jnp.clip(1.0 + 0.18 * jax.random.normal(keys[8], (HEADS, VALUE_DIM), jnp.float32), 0.1, 1.9),
        "out_weight": draw_out_weight(jax.random.fold_in(keys[16], 71), 0),
        "norm1_gain": jnp.clip(1.0 + 0.18 * jax.random.normal(keys[10], (D,), jnp.float32), 0.1, 1.9),
        "norm1_bias": scatter_about(keys[11], (D,), 0.5, 3.0, ((0, 64),), jnp.float32),
        "up_weight": scatter_about(keys[12], (D, MIXER_UNITS), D ** -0.5, 0.09375, ((1, 64),)),
        "down_weight": draw_down_weight(jax.random.fold_in(keys[16], 71), 0),
        "norm2_gain": jnp.clip(1.0 + 0.18 * jax.random.normal(keys[14], (D,), jnp.float32), 0.1, 1.9),
        "norm2_bias": scatter_about(keys[15], (D,), 0.5, 3.0, ((0, 64),), jnp.float32),
    }


ALPHA = 2.0 ** 0.5
TAU = 16.0
LN_EPS = 1e-05
RMS_EPS = 1e-06

def project(inputs, weight):
    flattened = weight.reshape(weight.shape[0], -1)
    return jnp.dot(inputs, flattened, preferred_element_type=jnp.float32).astype(jnp.bfloat16)

def normalize(inputs, row_gain, row_shift):
    average = lax.optimization_barrier(jnp.sum(inputs, axis=-1, keepdims=True)) / inputs.shape[-1]
    spread = lax.optimization_barrier(jnp.sum(inputs * inputs, axis=-1, keepdims=True)) / inputs.shape[-1] - average * average
    return ((inputs - average) * lax.rsqrt(spread + LN_EPS) * row_gain + row_shift).astype(jnp.bfloat16)

def reference(tokens, query_weight, key_weight, value_weight, gate_weight, decay_weight, decay_bias, states, head_gain, out_weight, norm1_gain, norm1_bias, up_weight, down_weight, norm2_gain, norm2_bias):
    row_count = tokens.shape[0]
    query_rows = project(tokens, query_weight).astype(jnp.float32).reshape(row_count, HEADS, KEY_DIM) * KEY_DIM ** (-0.5)
    key_rows = project(tokens, key_weight).astype(jnp.float32).reshape(row_count, HEADS, KEY_DIM)
    decay_rows = project(tokens, decay_weight).astype(jnp.float32).reshape(row_count, HEADS, KEY_DIM)
    value_rows = project(tokens, value_weight).astype(jnp.float32).reshape(row_count, HEADS, VALUE_DIM)
    gate_rows = project(tokens, gate_weight).astype(jnp.float32).reshape(row_count, HEADS, VALUE_DIM)
    retain = jnp.exp(jax.nn.log_sigmoid(decay_rows + decay_bias) / TAU)
    new_states = retain[..., None] * states + key_rows[..., :, None] * value_rows[..., None, :]
    readout = jnp.einsum('rhk,rhkv->rhv', query_rows, new_states, precision=lax.Precision.HIGHEST)
    readout = readout * lax.rsqrt(lax.optimization_barrier(jnp.mean(readout * readout, axis=-1, keepdims=True)) + RMS_EPS) * head_gain
    attended = (readout * jax.nn.silu(gate_rows)).astype(jnp.bfloat16).reshape(row_count, HEADS * VALUE_DIM)
    mixed_heads = jnp.dot(attended, out_weight, preferred_element_type=jnp.float32)
    residual_one = ALPHA * tokens.astype(jnp.float32) + mixed_heads
    normed = normalize(residual_one, norm1_gain, norm1_bias)
    lifted = jnp.dot(normed, up_weight, preferred_element_type=jnp.float32)
    hidden = jnp.square(jax.nn.relu(lifted)).astype(jnp.bfloat16)
    residual_two = ALPHA * normed.astype(jnp.float32) + jnp.dot(hidden, down_weight, preferred_element_type=jnp.float32)
    return (normalize(residual_two, norm2_gain, norm2_bias), new_states)
```

```python
import functools

import jax
import jax.numpy as jnp
from jax import lax
from jax.experimental import pallas as pl
from jax.experimental.pallas import tpu as pltpu
from jax.sharding import PartitionSpec as P

D = 4096
KEY_DIM = 128
ALPHA = 2.0**0.5
TAU = 16.0
LN_EPS = 1e-05
RMS_EPS = 1e-06
MESH = pl.DeviceIdType.MESH
F32 = jnp.float32
BF16 = jnp.bfloat16
NT = (((1,), (1,)), ((), ()))
NN = (((1,), (0,)), ((), ()))
TN = (((0,), (0,)), ((), ()))
CHIPS = 32


def dot(a, b, dims):
    return lax.dot_general(a, b, dims, preferred_element_type=F32)


def iota(shape, dim):
    return lax.broadcasted_iota(jnp.int32, shape, dim)


def kernel(
    tok, wq, wk, wd, wv, wg, bias, states, head_gain, ow, g1, b1, up, dn, g2, b2,
    out, new_states,
    wst, wc, owc, upc, dnc, st,
    s_a, r_a, s_g, r_g, x, s_b, r_b, ro, s_c, r_c, att32, att,
    s_e, r_e, s_m, r_m, xt, xn, s_y, r_y, s_h, r_h, s_f, r_f, sq,
    own_sem, w_send, w_recv, st_out_sem,
    a_sem, g_sem, b_sem, c_sem, e_sem, m_sem, y_sem, h_sem, f_sem,
):
    kv = lax.axis_index("kv")
    t = lax.axis_index("tp")
    z, xx = kv // 4, kv % 4
    half = kv // 16
    mine = half == t

    def chip_at(j):
        i = j // 4
        dz = lax.rem(4 + ((i + 1) // 2) * (2 * lax.rem(i, 2) - 1) + 8, 8)
        dx = lax.rem(j + 1, 4)
        return lax.rem(z + dz, 8) * 4 + lax.rem(xx + dx, 4)

    def rcopy(src, dst, sems, kv_to, t_to):
        return pltpu.make_async_remote_copy(
            src_ref=src, dst_ref=dst, send_sem=sems.at[0], recv_sem=sems.at[1],
            device_id={"kv": kv_to, "tp": t_to}, device_id_type=MESH,
        )

    def drain(ref, sem):
        pltpu.make_async_copy(ref, ref, sem).wait()

    own = [
        pltpu.make_async_copy(wq, wst.at[t, 0], own_sem.at[0]),
        pltpu.make_async_copy(wk, wst.at[t, 1], own_sem.at[1]),
        pltpu.make_async_copy(wd, wst.at[t, 2], own_sem.at[2]),
        pltpu.make_async_copy(wv, wc.at[t, pl.ds(96, 64)], own_sem.at[3]),
        pltpu.make_async_copy(wg, wc.at[t, pl.ds(160, 64)], own_sem.at[4]),
        pltpu.make_async_copy(states, st, own_sem.at[5]),
        pltpu.make_async_copy(ow, owc.at[t], own_sem.at[6]),
        pltpu.make_async_copy(up, upc.at[t], own_sem.at[7]),
        pltpu.make_async_copy(dn, dnc.at[t], own_sem.at[8]),
    ]
    for c in own:
        c.start()

    barrier = pltpu.get_barrier_semaphore()

    @pl.loop(1, 64)
    def _(i):
        p = lax.rem(kv * 2 + t + i, 64)
        pl.semaphore_signal(barrier, inc=1, device_id={"kv": p // 2, "tp": lax.rem(p, 2)}, device_id_type=MESH)

    tk = tok[...].astype(F32)
    for hh in range(2):
        s_a[hh] = jnp.concatenate(
            [tk[32 * hh : 32 * hh + 16], tk[32 * hh + 16 : 32 * hh + 32]], axis=1
        ).astype(BF16)
    s_g[0:1] = jnp.concatenate([g1[...], b1[...]], axis=1)
    s_g[1:2] = jnp.concatenate([g2[...], b2[...]], axis=1)
    me = t * CHIPS + kv
    r_a[me] = s_a[t]
    r_g[me] = s_g[...]
    pl.semaphore_wait(barrier, 63)

    @pl.loop(0, CHIPS)
    def _(j):
        kp = chip_at(j)
        for tt in range(2):

            @pl.when(jnp.logical_or(kp != kv, t != tt))
            def _():
                rcopy(s_a.at[tt], r_a.at[me], a_sem, kp, tt).start()

    partner = 1 - t

    def wcopy(src, dst, i):
        return pltpu.make_async_remote_copy(
            src_ref=src, dst_ref=dst, send_sem=w_send.at[i], recv_sem=w_recv.at[i],
            device_id={"kv": kv, "tp": partner}, device_id_type=MESH,
        )

    wcopies = [
        wcopy(wq, wst.at[t, 0], 0),
        wcopy(wk, wst.at[t, 1], 1),
        wcopy(wd, wst.at[t, 2], 2),
        wcopy(wv, wc.at[t, pl.ds(96, 64)], 3),
        wcopy(wg, wc.at[t, pl.ds(160, 64)], 4),
        wcopy(ow, owc.at[t], 5),
        wcopy(up, upc.at[t], 6),
        wcopy(dn, dnc.at[t], 7),
    ]
    for c in wcopies[:5]:
        c.start()

    @pl.loop(0, CHIPS)
    def _(j):
        kp = chip_at(j)
        for tt in range(2):

            @pl.when(jnp.logical_or(kp != kv, t != tt))
            def _():
                rcopy(s_g, r_g.at[me], g_sem, kp, tt).start()

    lane = iota((16, 128), 1) < 64
    col = iota((224, 256), 1)
    row = iota((224, 256), 0)
    low = col < 128
    j2 = col - 128
    src_low = ((col % 32) // 8) * 32 + (col % 8) * 4 + col // 32
    src_high = 96 + ((j2 % 16) // 8) * 64 + (j2 % 8) * 8 + j2 // 16
    src_low = jnp.where(col % 32 < 24, src_low, -1)
    perm = jnp.where(row == jnp.where(low, src_low, src_high), 1.0, 0.0).astype(BF16)
    e1 = jnp.where(iota((128, 128), 1) == (iota((128, 128), 0) % 4) * 32 + iota((128, 128), 0) // 4, 1.0, 0.0).astype(BF16)
    e2 = jnp.where(iota((256, 256), 0) == (iota((256, 256), 1) % 8) * 32 + iota((256, 256), 1) // 8, 1.0, 0.0).astype(BF16)
    zero = lambda n: jnp.zeros((n, 128), F32)
    bias_full = jnp.concatenate(
        [zero(16), bias[...], zero(24), bias[...], zero(8 + 64)], axis=0
    ).T[:, :64]

    for c in own:
        c.wait()
    for c in wcopies[:5]:
        c.wait()
    for c in wcopies[5:]:
        c.start()
    for tt in range(2):
        for ty in range(3):
            for h in range(0, 8, 4):
                wc[tt, ty * 32 + h * 4 : ty * 32 + h * 4 + 16, :] = jnp.concatenate(
                    [wst[tt, ty, h + i].astype(F32) for i in range(4)], axis=0
                ).astype(BF16)

    drain(r_a.at[pl.ds(0, 63)], a_sem.at[1])
    for c in range(CHIPS):
        a0 = r_a[c].astype(F32)
        a1 = r_a[CHIPS + c].astype(F32)
        x[0:16, c * 128 : (c + 1) * 128] = jnp.where(lane, a0, pltpu.roll(a1, 64, 1)).astype(BF16)
        x[16:32, c * 128 : (c + 1) * 128] = jnp.where(lane, pltpu.roll(a0, 64, 1), a1).astype(BF16)

    for tt in range(2):
        p = dot(x[...], wc[tt], NT).astype(BF16)
        p = dot(p, perm, NN)
        for i in range(16):
            s_b[i, tt] = p[2 * i : 2 * i + 2, :]

    @pl.loop(0, 16)
    def _(i):
        k16 = lax.rem(kv + 8 + i, 16)
        kp = 16 * t + k16
        for tt in range(2):

            @pl.when(jnp.logical_or(kp != kv, t != tt))
            def _():
                rcopy(s_b.at[k16, tt], r_b.at[kv], b_sem, kp, tt).start()

    @pl.when(mine)
    def _():
        r_b[kv] = s_b[lax.rem(kv, 16), t]
        drain(r_b.at[pl.ds(0, 31)], b_sem.at[1])

    @pl.when(jnp.logical_not(mine))
    def _():
        drain(r_b, b_sem.at[1])

    qkd, vg = [], []
    for s in range(2):
        rs = r_b[:, s, :]
        qkd.append(jnp.concatenate([rs[:, c * 32 : (c + 1) * 32] for c in range(4)], axis=0))
        vg.append(jnp.concatenate([rs[:, 128 + c * 16 : 144 + c * 16] for c in range(8)], axis=0))
    cols = dot(e1, jnp.concatenate(qkd, axis=1).astype(BF16), NN)
    rows = [dot(v.astype(BF16), e2, TN) for v in vg]
    decay = cols + bias_full
    log_sig = jnp.minimum(decay, 0.0) - jnp.log1p(jnp.exp(-jnp.abs(decay)))
    retain = jnp.exp(log_sig / TAU)
    q = cols * KEY_DIM ** (-0.5)
    for s in range(2):
        for h in range(8):
            o = s * 32 + h
            new = retain[:, o + 16 : o + 17] * st[s, h] + cols[:, o + 8 : o + 9] * rows[s][h : h + 1, :]
            st[s, h] = new
            ro[s * 8 + h : s * 8 + h + 1, :] = jnp.sum(q[:, o : o + 1] * new, axis=0, keepdims=True)
    st_out = pltpu.make_async_copy(st, new_states, st_out_sem)
    st_out.start()
    readout = ro[...]
    gate = jnp.concatenate([rows[0][8:16], rows[1][8:16]], axis=0)
    hg = jnp.concatenate([head_gain[...], head_gain[...]], axis=0)
    readout = readout * lax.rsqrt(jnp.mean(readout * readout, axis=-1, keepdims=True) + RMS_EPS) * hg
    s_c[...] = (readout * (gate / (1.0 + jnp.exp(-gate)))).astype(BF16)

    slot_c = t * 16 + lax.rem(kv, 16)

    @pl.loop(0, CHIPS)
    def _(j):
        kp = chip_at(j)

        @pl.when(jnp.logical_or(kp != kv, t != half))
        def _():
            rcopy(s_c, r_c.at[slot_c], c_sem, kp, half).start()

    @pl.when(mine)
    def _():
        r_c[slot_c] = s_c[...]
        drain(r_c.at[pl.ds(0, 31)], c_sem.at[1])

    @pl.when(jnp.logical_not(mine))
    def _():
        drain(r_c, c_sem.at[1])

    for tt in range(2):
        arrived = r_c[tt * 16 : (tt + 1) * 16].astype(F32).reshape(256, 256)
        for n in range(2):
            att32[n] = arrived[:, n * 128 : (n + 1) * 128]
            for h in range(8):
                at = tt * 2048 + h * 256 + n * 128
                att[:, at : at + 128] = att32[n, pl.ds(h, 32, stride=8), :].astype(BF16)
    wcopies[5].wait()
    mixed = jnp.concatenate([dot(att[...], owc[tt], NT) for tt in range(2)], axis=1)
    at_chip = pl.multiple_of(kv * 128, 128)
    res1 = ALPHA * x[:, pl.ds(at_chip, 128)].astype(F32) + mixed

    m_own = jnp.mean(res1, axis=-1, keepdims=True)
    sq[0:32, :] = jnp.broadcast_to(m_own, (32, 128))
    sq[32:128, :] = jnp.zeros((96, 128), F32)
    s_m[...] = sq[...].T[0:1, :]
    s_e[...] = (res1 - m_own).astype(BF16)

    @pl.loop(0, CHIPS - 1)
    def _(j):
        kp = chip_at(j)
        rcopy(s_e, r_e.at[kv], e_sem, kp, t).start()
        rcopy(s_m, r_m.at[kv], m_sem, kp, t).start()

    r_e[kv] = s_e[...]
    r_m[kv] = s_m[...]
    drain(r_g.at[pl.ds(0, 63)], g_sem.at[1])
    ga = r_g[0:32, 0, :]
    gb = r_g[32:64, 0, :]
    lane32 = iota((32, 128), 1) < 64
    gain1 = jnp.where(lane32, ga, pltpu.roll(gb, 64, 1))
    bias1 = jnp.where(lane32, pltpu.roll(ga, 64, 1), gb)
    wcopies[6].wait()
    wcopies[7].wait()
    drain(r_m.at[pl.ds(0, 31)], m_sem.at[1])
    drain(r_e.at[pl.ds(0, 31)], e_sem.at[1])
    sq[0:32, :] = r_m[:, 0, :]
    means = sq[...].T[0:32, 0:32]
    acc = jnp.zeros((32, 128), F32)
    for c in range(CHIPS):
        acc = acc + r_e[c].astype(F32)
    mean = (jnp.sum(acc, axis=-1, keepdims=True) + 128.0 * jnp.sum(means, axis=-1, keepdims=True)) / D
    acc = jnp.zeros((32, 128), F32)
    for c in range(CHIPS):
        v = r_e[c].astype(F32) + (means[:, c : c + 1] - mean)
        xt[c] = v
        acc = acc + v * v
    inv = lax.rsqrt(jnp.sum(acc, axis=-1, keepdims=True) / D + LN_EPS)
    for c in range(CHIPS):
        xn[:, c * 128 : (c + 1) * 128] = (xt[c] * inv * gain1[c : c + 1, :] + bias1[c : c + 1, :]).astype(BF16)

    hidden = []
    for tt in range(2):
        lifted = jnp.maximum(dot(xn[...], upc[tt], NN), 0.0)
        hidden.append((lifted * lifted).astype(BF16))

    @pl.loop(0, CHIPS)
    def _(j):
        kp = chip_at(j)
        cl = pl.ds(pl.multiple_of(kp * 128, 128), 128)
        y = dot(hidden[0], dnc[0, :, cl], NN) + dot(hidden[1], dnc[1, :, cl], NN)
        s_y[kp] = y.astype(BF16)

        @pl.when(kp != kv)
        def _():
            rcopy(s_y.at[kp], r_y.at[kv], y_sem, kp, t).start()

    r_y[kv] = s_y[kv]
    drain(r_y.at[pl.ds(0, 31)], y_sem.at[1])
    res2 = ALPHA * xn[:, pl.ds(at_chip, 128)].astype(F32)
    for c in range(CHIPS):
        res2 = res2 + r_y[c].astype(F32)

    m_own = jnp.mean(res2, axis=-1, keepdims=True)
    dev = res2 - m_own
    v_own = jnp.sum(dev * dev, axis=-1, keepdims=True)
    sq[0:32, :] = jnp.where(iota((32, 128), 1) == 0, m_own, v_own)
    s_h[...] = sq[...].T[0:2, :]

    @pl.loop(0, CHIPS - 1)
    def _(j):
        rcopy(s_h, r_h.at[kv], h_sem, chip_at(j), t).start()

    r_h[kv] = s_h[...]
    drain(r_h.at[pl.ds(0, 31)], h_sem.at[1])
    ms = r_h[:, 0, :]
    vs = r_h[:, 1, :]
    mean = jnp.mean(ms, axis=0, keepdims=True)
    dm = ms - mean
    spread = (jnp.sum(vs, axis=0, keepdims=True) + 128.0 * jnp.sum(dm * dm, axis=0, keepdims=True)) / D
    inv = lax.rsqrt(spread + LN_EPS)
    sq[0:1, :] = mean
    sq[1:2, :] = inv
    back = sq[...].T
    own0 = r_g[kv][1:2, :]
    own1 = r_g[CHIPS + kv][1:2, :]
    lane1 = iota((1, 128), 1) < 64
    gain2 = jnp.where(lane1, own0, pltpu.roll(own1, 64, 1))
    bias2 = jnp.where(lane1, pltpu.roll(own0, 64, 1), own1)
    o = ((res2 - back[0:32, 0:1]) * back[0:32, 1:2] * gain2 + bias2)
    s_f[...] = o.astype(BF16)
    last = rcopy(s_f, r_f, f_sem, kv, partner)
    last.start()
    first = t == 0
    out[pl.ds(pl.multiple_of(t * 32, 32), 32), :] = jnp.where(first, o, pltpu.roll(o, 64, 1))[:, :64].astype(BF16)
    last.wait()
    f = r_f[...].astype(F32)
    out[pl.ds(pl.multiple_of(partner * 32, 32), 32), :] = jnp.where(first, f, pltpu.roll(f, 64, 1))[:, :64].astype(BF16)

    drain(r_a.at[pl.ds(0, 63)], a_sem.at[0])
    drain(r_g.at[pl.ds(0, 63)], g_sem.at[0])

    @pl.when(mine)
    def _():
        drain(r_b.at[pl.ds(0, 31)], b_sem.at[0])
        drain(r_c.at[pl.ds(0, 31)], c_sem.at[0])

    @pl.when(jnp.logical_not(mine))
    def _():
        drain(r_b, b_sem.at[0])
        drain(r_c, c_sem.at[0])

    drain(r_e.at[pl.ds(0, 31)], e_sem.at[0])
    drain(r_m.at[pl.ds(0, 31)], m_sem.at[0])
    drain(r_y.at[pl.ds(0, 31)], y_sem.at[0])
    drain(r_h.at[pl.ds(0, 31)], h_sem.at[0])
    st_out.wait()


def body(
    tokens, query_weight, key_weight, value_weight, gate_weight, decay_weight, decay_bias, states,
    head_gain, out_weight, norm1_gain, norm1_bias, up_weight, down_weight, norm2_gain, norm2_bias,
):
    flip = lambda w: w.transpose(1, 2, 0)
    flat = lambda w: flip(w).reshape(-1, D)
    line = lambda v: v.reshape(1, -1)
    vmem = pl.BlockSpec(memory_space=pltpu.VMEM)
    hbm = pl.BlockSpec(memory_space=pl.ANY)
    V = pltpu.VMEM
    dma = pltpu.SemaphoreType.DMA
    scratch = [
        V((2, 3, 8, 4, D), BF16),
        V((2, 224, D), BF16),
        V((2, 64, D), BF16),
        V((2, D, 256), BF16),
        V((2, 256, D), BF16),
        V((2, 8, 128, 256), F32),
        V((2, 16, 128), BF16), V((64, 16, 128), BF16),
        V((2, 128), F32), V((64, 2, 128), F32),
        V((32, D), BF16),
        V((16, 2, 2, 256), F32), V((32, 2, 256), F32),
        V((16, 256), F32),
        V((16, 256), BF16), V((32, 16, 256), BF16),
        V((2, 256, 128), F32), V((32, D), BF16),
        V((32, 128), BF16), V((32, 32, 128), BF16),
        V((1, 128), F32), V((32, 1, 128), F32),
        V((32, 32, 128), F32), V((32, D), BF16),
        V((32, 32, 128), BF16), V((32, 32, 128), BF16),
        V((2, 128), F32), V((32, 2, 128), F32),
        V((32, 128), BF16), V((32, 128), BF16),
        V((128, 128), F32),
        dma((9,)), dma((8,)), dma((8,)), dma,
    ] + [dma((2,))] * 9
    return pl.pallas_call(
        kernel,
        out_shape=(
            jax.ShapeDtypeStruct((64, 64), BF16),
            jax.ShapeDtypeStruct((2, 8, 128, 256), F32),
        ),
        in_specs=[vmem] + [hbm] * 5 + [vmem, hbm, vmem, hbm, vmem, vmem, hbm, hbm, vmem, vmem],
        out_specs=(vmem, hbm),
        scratch_shapes=scratch,
        compiler_params=pltpu.CompilerParams(
            collective_id=0, has_side_effects=True, vmem_limit_bytes=60 * 1024 * 1024
        ),
        name="layer_step",
    )(
        tokens, flip(query_weight), flip(key_weight), flip(decay_weight), flat(value_weight), flat(gate_weight),
        decay_bias, states, head_gain, out_weight.T, line(norm1_gain), line(norm1_bias), up_weight, down_weight,
        line(norm2_gain), line(norm2_bias),
    )


def solution(mesh):
    placed = (
        P("dp", ("kv", "tp")),
        P(None, "tp", "kv"),
        P(None, "tp", "kv"),
        P(None, "tp", "kv"),
        P(None, "tp", "kv"),
        P(None, "tp", "kv"),
        P("tp", None),
        P(("dp", "kv"), "tp", None, None),
        P("tp", None),
        P(None, ("kv", "tp")),
        P(("kv", "tp")),
        P(("kv", "tp")),
        P(None, ("kv", "tp")),
        P(("kv", "tp"), None),
        P(("kv", "tp")),
        P(("kv", "tp")),
    )
    return jax.shard_map(
        body,
        mesh=mesh,
        in_specs=placed,
        out_specs=(P("dp", ("kv", "tp")), P(("dp", "kv"), "tp", None, None)),
        check_vma=False,
    )
```

```python
import functools

import jax
import jax.numpy as jnp
from jax import lax
from jax.experimental import pallas as pl
from jax.experimental.pallas import tpu as pltpu
from jax.sharding import PartitionSpec as P

D = 4096
KEY_DIM = 128
ALPHA = 2.0**0.5
TAU = 16.0
LN_EPS = 1e-05
RMS_EPS = 1e-06
MESH = pl.DeviceIdType.MESH
F32 = jnp.float32
BF16 = jnp.bfloat16
NT = (((1,), (1,)), ((), ()))
NN = (((1,), (0,)), ((), ()))
TN = (((0,), (0,)), ((), ()))
CHIPS = 32
FAR = sorted(
    ((d, e) for d in range(8) for e in range(4) if d or e),
    key=lambda o: (-min(o[0], 8 - o[0]) - min(o[1], 4 - o[1]), o),
)


def dot(a, b, dims):
    return lax.dot_general(a, b, dims, preferred_element_type=F32)


def iota(shape, dim):
    return lax.broadcasted_iota(jnp.int32, shape, dim)


def kernel(
    tok, wq, wk, wd, wv, wg, bias, states, head_gain, ow, g1, b1, up, dn, g2, b2,
    out, new_states,
    wst, wc, owc, upc, dnc, st,
    s_a, r_a, s_g, r_g, x, s_b, r_b, ro, s_c, r_c, att32, att,
    s_e, r_e, s_m, r_m, xt, xn, s_y, r_y, s_h, r_h, s_f, r_f, sq,
    own_sem, w_send, w_recv,
    az_send, az_recv, ax_sem, g_sem, p_sem, b_sem, c_sem, e_sem, m_sem, y_sem, h_sem, f_sem,
):
    kv = lax.axis_index("kv")
    t = lax.axis_index("tp")
    z, xx = kv // 4, kv % 4
    half = kv // 16
    mine = half == t
    partner = 1 - t

    def wrap(v, n):
        return jnp.where(v >= n, v - n, v)

    zd = [wrap(z + d, 8) for d in range(8)]
    xd = [wrap(xx + d, 4) for d in range(4)]

    def rcopy(src, dst, sems, kv_to, t_to):
        return pltpu.make_async_remote_copy(
            src_ref=src, dst_ref=dst, send_sem=sems.at[0], recv_sem=sems.at[1],
            device_id={"kv": kv_to, "tp": t_to}, device_id_type=MESH,
        )

    def drain(ref, sem):
        pltpu.make_async_copy(ref, ref, sem).wait()

    own = [
        pltpu.make_async_copy(wq, wst.at[0], own_sem.at[0]),
        pltpu.make_async_copy(wk, wst.at[1], own_sem.at[1]),
        pltpu.make_async_copy(wd, wst.at[2], own_sem.at[2]),
        pltpu.make_async_copy(wv, wc.at[t, pl.ds(96, 64)], own_sem.at[3]),
        pltpu.make_async_copy(wg, wc.at[t, pl.ds(160, 64)], own_sem.at[4]),
        pltpu.make_async_copy(states, st, own_sem.at[5]),
        pltpu.make_async_copy(ow, owc.at[t], own_sem.at[6]),
        pltpu.make_async_copy(up, upc.at[t], own_sem.at[7]),
        pltpu.make_async_copy(dn, dnc.at[t], own_sem.at[8]),
    ]
    for c in own:
        c.start()

    barrier = pltpu.get_barrier_semaphore()

    def hello(kv_to, t_to):
        pl.semaphore_signal(barrier, inc=1, device_id={"kv": kv_to, "tp": t_to}, device_id_type=MESH)

    for d in (4, 3, 5, 2, 6, 1, 7):
        hello(zd[d] * 4 + xx, t)
        hello(zd[d] * 4 + xx, partner)
    for d in (2, 1, 3):
        hello(z * 4 + xd[d], t)
    hello(kv, partner)

    tk = tok[...].astype(F32)
    for hh in range(2):
        s_a[hh] = jnp.concatenate(
            [tk[32 * hh : 32 * hh + 16], tk[32 * hh + 16 : 32 * hh + 32]], axis=1
        ).astype(BF16)
    s_g[0:1] = jnp.concatenate([g1[...], b1[...]], axis=1)
    s_g[1:2] = jnp.concatenate([g2[...], b2[...]], axis=1)
    me = kv * 2 + t
    r_a[me] = s_a[t]
    r_g[t, kv] = s_g[...]

    lane = iota((16, 128), 1) < 64
    col = iota((224, 256), 1)
    row = iota((224, 256), 0)
    low = col < 128
    j2 = col - 128
    src_low = ((col % 32) // 8) * 32 + (col % 8) * 4 + col // 32
    src_high = 96 + ((j2 % 16) // 8) * 64 + (j2 % 8) * 8 + j2 // 16
    src_low = jnp.where(col % 32 < 24, src_low, -1)
    perm = jnp.where(row == jnp.where(low, src_low, src_high), 1.0, 0.0).astype(BF16)
    e1 = jnp.where(iota((128, 128), 1) == (iota((128, 128), 0) % 4) * 32 + iota((128, 128), 0) // 4, 1.0, 0.0).astype(BF16)
    e2 = jnp.where(iota((256, 256), 0) == (iota((256, 256), 1) % 8) * 32 + iota((256, 256), 1) // 8, 1.0, 0.0).astype(BF16)
    zero = lambda n: jnp.zeros((n, 128), F32)
    bias_full = jnp.concatenate(
        [zero(16), bias[...], zero(24), bias[...], zero(8 + 64)], axis=0
    ).T[:, :64]

    for c in own[:5]:
        c.wait()
    for ty in range(3):
        for h in range(0, 8, 4):
            wc[t, ty * 32 + h * 4 : ty * 32 + h * 4 + 16, :] = jnp.concatenate(
                [wst[ty, h + i].astype(F32) for i in range(4)], axis=0
            ).astype(BF16)

    def wcopy(ref, i):
        return pltpu.make_async_remote_copy(
            src_ref=ref.at[t], dst_ref=ref.at[t], send_sem=w_send.at[i], recv_sem=w_recv.at[i],
            device_id={"kv": kv, "tp": partner}, device_id_type=MESH,
        )

    wcopies = [wcopy(wc, 0), wcopy(owc, 1), wcopy(upc, 2), wcopy(dnc, 3)]
    pl.semaphore_wait(barrier, 18)

    def to_line(src, kv_to, t_to):
        pltpu.make_async_remote_copy(
            src_ref=src, dst_ref=r_a.at[me], send_sem=az_send, recv_sem=az_recv.at[z * 2 + t],
            device_id={"kv": kv_to, "tp": t_to}, device_id_type=MESH,
        ).start()

    to_line(s_a.at[partner], kv, partner)
    for d in (4, 3, 5, 2, 6, 1, 7):
        for tt in range(2):
            to_line(s_a.at[tt], zd[d] * 4 + xx, tt)
    wcopies[0].start()
    for d in (0, 1, 7, 2, 6, 3, 5, 4):
        if d == 0:
            drain(r_a.at[0], az_recv.at[z * 2 + partner])
        else:
            drain(r_a.at[0], az_recv.at[zd[d] * 2])
            drain(r_a.at[0], az_recv.at[zd[d] * 2 + 1])
        block = r_a.at[pl.ds((zd[d] * 4 + xx) * 2, 2)]
        for e in (2, 1, 3):
            rcopy(block, block, ax_sem, z * 4 + xd[e], t).start()
    drain(r_a.at[pl.ds(0, 48)], ax_sem.at[1])
    for c in range(CHIPS):
        a0 = r_a[2 * c].astype(F32)
        a1 = r_a[2 * c + 1].astype(F32)
        x[0:16, c * 128 : (c + 1) * 128] = jnp.where(lane, a0, pltpu.roll(a1, 64, 1)).astype(BF16)
        x[16:32, c * 128 : (c + 1) * 128] = jnp.where(lane, pltpu.roll(a0, 64, 1), a1).astype(BF16)

    wcopies[0].wait()
    for tt in range(2):
        p = dot(x[...], wc[tt], NT).astype(BF16)
        p = dot(p, perm, NN)
        for i in range(16):
            s_b[i, tt] = p[2 * i : 2 * i + 2, :]

    for i in range(4):
        zl = wrap(z - 4 * half + i, 4)
        for j in (2, 1, 3, 0):
            k16 = zl * 4 + xd[j]
            kp = 16 * t + k16
            for tt in range(2):
                if i == 0 and j == 0:

                    @pl.when(jnp.logical_not(jnp.logical_and(mine, t == tt)))
                    def _():
                        rcopy(s_b.at[k16, tt], r_b.at[kv], b_sem, kp, tt).start()

                else:
                    rcopy(s_b.at[k16, tt], r_b.at[kv], b_sem, kp, tt).start()

    for i in range(1, 4):
        own[5 + i].wait()
        wcopies[i].start()
    for d, e in FAR:
        rcopy(s_g, r_g.at[t, kv], g_sem, zd[d] * 4 + xd[e], t).start()
    own[5].wait()

    @pl.when(mine)
    def _():
        r_b[kv] = s_b[lax.rem(kv, 16), t]
        drain(r_b.at[pl.ds(0, 31)], b_sem.at[1])

    @pl.when(jnp.logical_not(mine))
    def _():
        drain(r_b, b_sem.at[1])

    qkd, vg = [], []
    for s in range(2):
        rs = r_b[:, s, :]
        qkd.append(jnp.concatenate([rs[:, c * 32 : (c + 1) * 32] for c in range(4)], axis=0))
        vg.append(jnp.concatenate([rs[:, 128 + c * 16 : 144 + c * 16] for c in range(8)], axis=0))
    cols = dot(e1, jnp.concatenate(qkd, axis=1).astype(BF16), NN)
    rows = [dot(v.astype(BF16), e2, TN) for v in vg]
    decay = cols + bias_full
    log_sig = jnp.minimum(decay, 0.0) - jnp.log1p(jnp.exp(-jnp.abs(decay)))
    retain = jnp.exp(log_sig / TAU)
    q = cols * KEY_DIM ** (-0.5)
    for s in range(2):
        for h in range(8):
            o = s * 32 + h
            new = retain[:, o + 16 : o + 17] * st[s, h] + cols[:, o + 8 : o + 9] * rows[s][h : h + 1, :]
            new_states[s, h] = new
            ro[s * 8 + h : s * 8 + h + 1, :] = jnp.sum(q[:, o : o + 1] * new, axis=0, keepdims=True)
    readout = ro[...]
    gate = jnp.concatenate([rows[0][8:16], rows[1][8:16]], axis=0)
    hg = jnp.concatenate([head_gain[...], head_gain[...]], axis=0)
    readout = readout * lax.rsqrt(jnp.mean(readout * readout, axis=-1, keepdims=True) + RMS_EPS) * hg
    s_c[...] = (readout * (gate / (1.0 + jnp.exp(-gate)))).astype(BF16)

    slot_c = t * 16 + lax.rem(kv, 16)

    for d, e in FAR:
        rcopy(s_c, r_c.at[slot_c], c_sem, zd[d] * 4 + xd[e], half).start()

    @pl.when(jnp.logical_not(mine))
    def _():
        rcopy(s_c, r_c.at[slot_c], c_sem, kv, half).start()

    drain(r_g.at[t, pl.ds(0, 31)], g_sem.at[1])
    gains = rcopy(r_g.at[t], r_g.at[t], p_sem, kv, partner)
    gains.start()

    @pl.when(mine)
    def _():
        r_c[slot_c] = s_c[...]
        drain(r_c.at[pl.ds(0, 31)], c_sem.at[1])

    @pl.when(jnp.logical_not(mine))
    def _():
        drain(r_c, c_sem.at[1])

    for tt in range(2):
        arrived = r_c[tt * 16 : (tt + 1) * 16].astype(F32).reshape(256, 256)
        for n in range(2):
            att32[n] = arrived[:, n * 128 : (n + 1) * 128]
            for h in range(8):
                at = tt * 2048 + h * 256 + n * 128
                att[:, at : at + 128] = att32[n, pl.ds(h, 32, stride=8), :].astype(BF16)
    wcopies[1].wait()
    mixed = jnp.concatenate([dot(att[...], owc[tt], NT) for tt in range(2)], axis=1)
    at_chip = pl.multiple_of(kv * 128, 128)
    res1 = ALPHA * x[:, pl.ds(at_chip, 128)].astype(F32) + mixed

    m_own = jnp.mean(res1, axis=-1, keepdims=True)
    sq[0:32, :] = jnp.broadcast_to(m_own, (32, 128))
    sq[32:128, :] = jnp.zeros((96, 128), F32)
    s_m[...] = sq[...].T[0:1, :]
    s_e[...] = (res1 - m_own).astype(BF16)

    for d, e in FAR:
        kp = zd[d] * 4 + xd[e]
        rcopy(s_e, r_e.at[kv], e_sem, kp, t).start()
        rcopy(s_m, r_m.at[kv], m_sem, kp, t).start()

    r_e[kv] = s_e[...]
    r_m[kv] = s_m[...]
    gains.wait()
    ga = r_g[0, :, 0, :]
    gb = r_g[1, :, 0, :]
    lane32 = iota((32, 128), 1) < 64
    gain1 = jnp.where(lane32, ga, pltpu.roll(gb, 64, 1))
    bias1 = jnp.where(lane32, pltpu.roll(ga, 64, 1), gb)
    wcopies[2].wait()
    wcopies[3].wait()
    drain(r_m.at[pl.ds(0, 31)], m_sem.at[1])
    drain(r_e.at[pl.ds(0, 31)], e_sem.at[1])
    sq[0:32, :] = r_m[:, 0, :]
    means = sq[...].T[0:32, 0:32]
    acc = jnp.zeros((32, 128), F32)
    for c in range(CHIPS):
        acc = acc + r_e[c].astype(F32)
    mean = (jnp.sum(acc, axis=-1, keepdims=True) + 128.0 * jnp.sum(means, axis=-1, keepdims=True)) / D
    acc = jnp.zeros((32, 128), F32)
    for c in range(CHIPS):
        v = r_e[c].astype(F32) + (means[:, c : c + 1] - mean)
        xt[c] = v
        acc = acc + v * v
    inv = lax.rsqrt(jnp.sum(acc, axis=-1, keepdims=True) / D + LN_EPS)
    for c in range(CHIPS):
        xn[:, c * 128 : (c + 1) * 128] = (xt[c] * inv * gain1[c : c + 1, :] + bias1[c : c + 1, :]).astype(BF16)

    hidden = []
    for tt in range(2):
        lifted = jnp.maximum(dot(xn[...], upc[tt], NN), 0.0)
        hidden.append((lifted * lifted).astype(BF16))
    for d in (4, 3, 5, 2, 6, 1, 7, 0):
        cl = pl.ds(pl.multiple_of(zd[d] * 512, 512), 512)
        y = (dot(hidden[0], dnc[0, :, cl], NN) + dot(hidden[1], dnc[1, :, cl], NN)).astype(BF16)
        for j in range(4):
            s_y[zd[d] * 4 + j] = y[:, j * 128 : (j + 1) * 128]
        for e in (2, 1, 3, 0):
            if d or e:
                kp = zd[d] * 4 + xd[e]
                rcopy(s_y.at[kp], r_y.at[kv], y_sem, kp, t).start()

    r_y[kv] = s_y[kv]
    drain(r_y.at[pl.ds(0, 31)], y_sem.at[1])
    res2 = ALPHA * xn[:, pl.ds(at_chip, 128)].astype(F32)
    for c in range(CHIPS):
        res2 = res2 + r_y[c].astype(F32)

    m_own = jnp.mean(res2, axis=-1, keepdims=True)
    dev = res2 - m_own
    v_own = jnp.sum(dev * dev, axis=-1, keepdims=True)
    sq[0:32, :] = jnp.where(iota((32, 128), 1) == 0, m_own, v_own)
    s_h[...] = sq[...].T[0:2, :]

    for d, e in FAR:
        rcopy(s_h, r_h.at[kv], h_sem, zd[d] * 4 + xd[e], t).start()

    r_h[kv] = s_h[...]
    drain(r_h.at[pl.ds(0, 31)], h_sem.at[1])
    ms = r_h[:, 0, :]
    vs = r_h[:, 1, :]
    mean = jnp.mean(ms, axis=0, keepdims=True)
    dm = ms - mean
    spread = (jnp.sum(vs, axis=0, keepdims=True) + 128.0 * jnp.sum(dm * dm, axis=0, keepdims=True)) / D
    inv = lax.rsqrt(spread + LN_EPS)
    sq[0:1, :] = mean
    sq[1:2, :] = inv
    back = sq[...].T
    own0 = r_g[0, kv][1:2, :]
    own1 = r_g[1, kv][1:2, :]
    lane1 = iota((1, 128), 1) < 64
    gain2 = jnp.where(lane1, own0, pltpu.roll(own1, 64, 1))
    bias2 = jnp.where(lane1, pltpu.roll(own0, 64, 1), own1)
    o = ((res2 - back[0:32, 0:1]) * back[0:32, 1:2] * gain2 + bias2)
    s_f[...] = o.astype(BF16)
    last = rcopy(s_f, r_f, f_sem, kv, partner)
    last.start()
    first = t == 0
    out[pl.ds(pl.multiple_of(t * 32, 32), 32), :] = jnp.where(first, o, pltpu.roll(o, 64, 1))[:, :64].astype(BF16)
    last.wait()
    f = r_f[...].astype(F32)
    out[pl.ds(pl.multiple_of(partner * 32, 32), 32), :] = jnp.where(first, f, pltpu.roll(f, 64, 1))[:, :64].astype(BF16)

    drain(r_a.at[pl.ds(0, 15)], az_send)
    drain(r_a.at[pl.ds(0, 48)], ax_sem.at[0])
    drain(r_g.at[t, pl.ds(0, 31)], g_sem.at[0])

    @pl.when(mine)
    def _():
        drain(r_b.at[pl.ds(0, 31)], b_sem.at[0])
        drain(r_c.at[pl.ds(0, 31)], c_sem.at[0])

    @pl.when(jnp.logical_not(mine))
    def _():
        drain(r_b, b_sem.at[0])
        drain(r_c, c_sem.at[0])

    drain(r_e.at[pl.ds(0, 31)], e_sem.at[0])
    drain(r_m.at[pl.ds(0, 31)], m_sem.at[0])
    drain(r_y.at[pl.ds(0, 31)], y_sem.at[0])
    drain(r_h.at[pl.ds(0, 31)], h_sem.at[0])


def body(
    tokens, query_weight, key_weight, value_weight, gate_weight, decay_weight, decay_bias, states,
    head_gain, out_weight, norm1_gain, norm1_bias, up_weight, down_weight, norm2_gain, norm2_bias,
):
    flip = lambda w: w.transpose(1, 2, 0)
    flat = lambda w: flip(w).reshape(-1, D)
    line = lambda v: v.reshape(1, -1)
    vmem = pl.BlockSpec(memory_space=pltpu.VMEM)
    hbm = pl.BlockSpec(memory_space=pl.ANY)
    V = pltpu.VMEM
    dma = pltpu.SemaphoreType.DMA
    scratch = [
        V((3, 8, 4, D), BF16),
        V((2, 224, D), BF16),
        V((2, 64, D), BF16),
        V((2, D, 256), BF16),
        V((2, 256, D), BF16),
        V((2, 8, 128, 256), F32),
        V((2, 16, 128), BF16), V((64, 16, 128), BF16),
        V((2, 128), F32), V((2, 32, 2, 128), F32),
        V((32, D), BF16),
        V((16, 2, 2, 256), F32), V((32, 2, 256), F32),
        V((16, 256), F32),
        V((16, 256), BF16), V((32, 16, 256), BF16),
        V((2, 256, 128), F32), V((32, D), BF16),
        V((32, 128), BF16), V((32, 32, 128), BF16),
        V((1, 128), F32), V((32, 1, 128), F32),
        V((32, 32, 128), F32), V((32, D), BF16),
        V((32, 32, 128), BF16), V((32, 32, 128), BF16),
        V((2, 128), F32), V((32, 2, 128), F32),
        V((32, 128), BF16), V((32, 128), BF16),
        V((128, 128), F32),
        dma((9,)), dma((4,)), dma((4,)), dma, dma((16,)),
    ] + [dma((2,))] * 10
    return pl.pallas_call(
        kernel,
        out_shape=(
            pltpu.VMEM((64, 64), BF16),
            pltpu.VMEM((2, 8, 128, 256), F32),
        ),
        in_specs=[vmem] + [hbm] * 5 + [vmem, hbm, vmem, hbm, vmem, vmem, hbm, hbm, vmem, vmem],
        out_specs=(vmem, vmem),
        scratch_shapes=scratch,
        compiler_params=pltpu.CompilerParams(
            collective_id=0, has_side_effects=True, vmem_limit_bytes=60 * 1024 * 1024
        ),
        name="layer_step",
    )(
        tokens, flip(query_weight), flip(key_weight), flip(decay_weight), flat(value_weight), flat(gate_weight),
        decay_bias, states, head_gain, out_weight.T, line(norm1_gain), line(norm1_bias), up_weight, down_weight,
        line(norm2_gain), line(norm2_bias),
    )


def solution(mesh):
    placed = (
        P("dp", ("kv", "tp")),
        P(None, "tp", "kv"),
        P(None, "tp", "kv"),
        P(None, "tp", "kv"),
        P(None, "tp", "kv"),
        P(None, "tp", "kv"),
        P("tp", None),
        P(("dp", "kv"), "tp", None, None),
        P("tp", None),
        P(None, ("kv", "tp")),
        P(("kv", "tp")),
        P(("kv", "tp")),
        P(None, ("kv", "tp")),
        P(("kv", "tp"), None),
        P(("kv", "tp")),
        P(("kv", "tp")),
    )
    return jax.shard_map(
        body,
        mesh=mesh,
        in_specs=placed,
        out_specs=(P("dp", ("kv", "tp")), P(("dp", "kv"), "tp", None, None)),
        check_vma=False,
    )
```

```python
import functools

import jax
import jax.numpy as jnp
from jax import lax
from jax.experimental import pallas as pl
from jax.experimental.pallas import tpu as pltpu
from jax.sharding import PartitionSpec as P

D = 4096
KEY_DIM = 128
ALPHA = 2.0**0.5
TAU = 16.0
LN_EPS = 1e-05
RMS_EPS = 1e-06
MESH = pl.DeviceIdType.MESH
F32 = jnp.float32
BF16 = jnp.bfloat16
NT = (((1,), (1,)), ((), ()))
NN = (((1,), (0,)), ((), ()))
TN = (((0,), (0,)), ((), ()))
CHIPS = 32
FAR = sorted(
    ((d, e) for d in range(8) for e in range(4) if d or e),
    key=lambda o: (-min(o[0], 8 - o[0]) - min(o[1], 4 - o[1]), o),
)
NEAR = (1, 7, 2, 6)


def dot(a, b, dims):
    return lax.dot_general(a, b, dims, preferred_element_type=F32)


def iota(shape, dim):
    return lax.broadcasted_iota(jnp.int32, shape, dim)


def kernel(
    tok_h, wq, wk, wd, wv, wg, bias_h, states, head_gain_h, ow, g1_h, b1_h, up, dn, g2_h, b2_h,
    out, new_states,
    tok, bias, head_gain, g1, b1, g2, b2, wst, wc, owc, upc, dnc, st,
    s_a, r_a, s_g, r_g, x, s_b, r_b, ro, s_c, r_c, att32, att,
    s_e, r_e, s_m, r_m, xt, xn, s_y, r_y, s_h, r_h, s_f, r_f, sq,
    small_sem, own_sem, w_send, w_recv,
    az_send, az_recv, ax_send, ax_recv, g_sem, p_sem, b_sem, c_send, c_recv, e_send, e_recv, m_sem, y_sem, h_sem, f_sem,
):
    kv = lax.axis_index("kv")
    t = lax.axis_index("tp")
    z, xx = kv // 4, kv % 4
    half = kv // 16
    mine = half == t
    partner = 1 - t

    def wrap(v, n):
        return jnp.where(v >= n, v - n, v)

    zd = [wrap(z + d, 8) for d in range(8)]
    xd = [wrap(xx + d, 4) for d in range(4)]

    def rcopy(src, dst, sems, kv_to, t_to):
        return pltpu.make_async_remote_copy(
            src_ref=src, dst_ref=dst, send_sem=sems.at[0], recv_sem=sems.at[1],
            device_id={"kv": kv_to, "tp": t_to}, device_id_type=MESH,
        )

    def drain(ref, sem):
        pltpu.make_async_copy(ref, ref, sem).wait()

    barrier = pltpu.get_barrier_semaphore()

    def hello(kv_to, t_to):
        pl.semaphore_signal(barrier, inc=1, device_id={"kv": kv_to, "tp": t_to}, device_id_type=MESH)

    for d in (4, 3, 5, 2, 6, 1, 7):
        hello(zd[d] * 4 + xx, t)
        hello(zd[d] * 4 + xx, partner)
    for d in (2, 1, 3):
        hello(z * 4 + xd[d], t)
    hello(kv, partner)

    small = [
        pltpu.make_async_copy(a, b, small_sem.at[i])
        for i, (a, b) in enumerate(
            [(tok_h, tok), (bias_h, bias), (head_gain_h, head_gain), (g1_h, g1), (b1_h, b1), (g2_h, g2), (b2_h, b2)]
        )
    ]
    for c in small:
        c.start()

    own = [
        pltpu.make_async_copy(wq, wst.at[0], own_sem.at[0]),
        pltpu.make_async_copy(wk, wst.at[1], own_sem.at[1]),
        pltpu.make_async_copy(wd, wst.at[2], own_sem.at[2]),
        pltpu.make_async_copy(wv, wc.at[t, pl.ds(96, 64)], own_sem.at[3]),
        pltpu.make_async_copy(wg, wc.at[t, pl.ds(160, 64)], own_sem.at[4]),
        pltpu.make_async_copy(states, st, own_sem.at[5]),
        pltpu.make_async_copy(ow, owc.at[t], own_sem.at[6]),
        pltpu.make_async_copy(up, upc.at[t], own_sem.at[7]),
        pltpu.make_async_copy(dn, dnc.at[t], own_sem.at[8]),
    ]
    for c in own:
        c.start()

    for c in small:
        c.wait()
    tk = tok[...].astype(F32)
    for hh in range(2):
        s_a[hh] = jnp.concatenate(
            [tk[32 * hh : 32 * hh + 16], tk[32 * hh + 16 : 32 * hh + 32]], axis=1
        ).astype(BF16)
    s_g[0:1] = jnp.concatenate([g1[...], b1[...]], axis=1)
    s_g[1:2] = jnp.concatenate([g2[...], b2[...]], axis=1)
    me = kv * 2 + t
    r_a[me] = s_a[t]
    r_g[t, kv] = s_g[...]

    lane = iota((16, 128), 1) < 64
    col = iota((224, 256), 1)
    row = iota((224, 256), 0)
    low = col < 128
    j2 = col - 128
    src_low = ((col % 32) // 8) * 32 + (col % 8) * 4 + col // 32
    src_high = 96 + ((j2 % 16) // 8) * 64 + (j2 % 8) * 8 + j2 // 16
    src_low = jnp.where(col % 32 < 24, src_low, -1)
    perm = jnp.where(row == jnp.where(low, src_low, src_high), 1.0, 0.0).astype(BF16)
    e1 = jnp.where(iota((128, 128), 1) == (iota((128, 128), 0) % 4) * 32 + iota((128, 128), 0) // 4, 1.0, 0.0).astype(BF16)
    e2 = jnp.where(iota((256, 256), 0) == (iota((256, 256), 1) % 8) * 32 + iota((256, 256), 1) // 8, 1.0, 0.0).astype(BF16)
    zero = lambda n: jnp.zeros((n, 128), F32)
    bias_full = jnp.concatenate(
        [zero(16), bias[...], zero(24), bias[...], zero(8 + 64)], axis=0
    ).T[:, :64]

    for c in own[:5]:
        c.wait()
    for ty in range(3):
        for h in range(0, 8, 4):
            wc[t, ty * 32 + h * 4 : ty * 32 + h * 4 + 16, :] = jnp.concatenate(
                [wst[ty, h + i].astype(F32) for i in range(4)], axis=0
            ).astype(BF16)

    def wcopy(ref, i):
        return pltpu.make_async_remote_copy(
            src_ref=ref.at[t], dst_ref=ref.at[t], send_sem=w_send.at[i], recv_sem=w_recv.at[i],
            device_id={"kv": kv, "tp": partner}, device_id_type=MESH,
        )

    wcopies = [wcopy(wc, 0), wcopy(owc, 1), wcopy(upc, 2), wcopy(dnc, 3)]
    pl.semaphore_wait(barrier, 18)

    def to_line(src, kv_to, t_to):
        pltpu.make_async_remote_copy(
            src_ref=src, dst_ref=r_a.at[me], send_sem=az_send, recv_sem=az_recv.at[z * 2 + t],
            device_id={"kv": kv_to, "tp": t_to}, device_id_type=MESH,
        ).start()

    to_line(s_a.at[partner], kv, partner)
    for d in (4, 3, 5, 2, 6, 1, 7):
        for tt in range(2):
            to_line(s_a.at[tt], zd[d] * 4 + xx, tt)
    wcopies[0].start()
    for d in (0, 1, 7, 2, 6, 3, 5, 4):
        if d == 0:
            drain(r_a.at[0], az_recv.at[z * 2 + partner])
        else:
            drain(r_a.at[0], az_recv.at[zd[d] * 2])
            drain(r_a.at[0], az_recv.at[zd[d] * 2 + 1])
        block = r_a.at[pl.ds((zd[d] * 4 + xx) * 2, 2)]
        for e in (2, 1, 3):
            pltpu.make_async_remote_copy(
                src_ref=block, dst_ref=block, send_sem=ax_send, recv_sem=ax_recv.at[zd[d]],
                device_id={"kv": z * 4 + xd[e], "tp": t}, device_id_type=MESH,
            ).start()

    wcopies[0].wait()
    projected = [jnp.zeros((32, 224), F32) for _ in range(2)]
    for d in (0, 1, 7, 2, 6, 3, 5, 4):
        drain(r_a.at[pl.ds(0, 6)], ax_recv.at[zd[d]])
        tiles = []
        for j in range(4):
            a0 = r_a[zd[d] * 8 + 2 * j].astype(F32)
            a1 = r_a[zd[d] * 8 + 2 * j + 1].astype(F32)
            low = jnp.where(lane, a0, pltpu.roll(a1, 64, 1))
            high = jnp.where(lane, pltpu.roll(a0, 64, 1), a1)
            tiles.append(jnp.concatenate([low, high], axis=0).astype(BF16))
        tile = jnp.concatenate(tiles, axis=1)
        cl = pl.ds(pl.multiple_of(zd[d] * 512, 512), 512)
        x[:, cl] = tile
        for tt in range(2):
            projected[tt] = projected[tt] + dot(tile, wc[tt, :, cl], NT)
    for tt in range(2):
        p = projected[tt].astype(BF16)
        p = dot(p, perm, NN)
        for i in range(16):
            s_b[i, tt] = p[2 * i : 2 * i + 2, :]

    for i in range(4):
        zl = wrap(z - 4 * half + i, 4)
        for j in (2, 1, 3, 0):
            k16 = zl * 4 + xd[j]
            kp = 16 * t + k16
            for tt in range(2):
                if i == 0 and j == 0:

                    @pl.when(jnp.logical_not(jnp.logical_and(mine, t == tt)))
                    def _():
                        rcopy(s_b.at[k16, tt], r_b.at[kv], b_sem, kp, tt).start()

                else:
                    rcopy(s_b.at[k16, tt], r_b.at[kv], b_sem, kp, tt).start()

    for i in range(1, 4):
        own[5 + i].wait()
        wcopies[i].start()
    for d, e in FAR:
        rcopy(s_g, r_g.at[t, kv], g_sem, zd[d] * 4 + xd[e], t).start()
    own[5].wait()

    @pl.when(mine)
    def _():
        r_b[kv] = s_b[lax.rem(kv, 16), t]
        drain(r_b.at[pl.ds(0, 31)], b_sem.at[1])

    @pl.when(jnp.logical_not(mine))
    def _():
        drain(r_b, b_sem.at[1])

    qkd, vg = [], []
    for s in range(2):
        rs = r_b[:, s, :]
        qkd.append(jnp.concatenate([rs[:, c * 32 : (c + 1) * 32] for c in range(4)], axis=0))
        vg.append(jnp.concatenate([rs[:, 128 + c * 16 : 144 + c * 16] for c in range(8)], axis=0))
    cols = dot(e1, jnp.concatenate(qkd, axis=1).astype(BF16), NN)
    rows = [dot(v.astype(BF16), e2, TN) for v in vg]
    decay = cols + bias_full
    log_sig = jnp.minimum(decay, 0.0) - jnp.log1p(jnp.exp(-jnp.abs(decay)))
    retain = jnp.exp(log_sig / TAU)
    q = cols * KEY_DIM ** (-0.5)
    for s in range(2):
        for h in range(8):
            o = s * 32 + h
            new = retain[:, o + 16 : o + 17] * st[s, h] + cols[:, o + 8 : o + 9] * rows[s][h : h + 1, :]
            new_states[s, h] = new
            ro[s * 8 + h : s * 8 + h + 1, :] = jnp.sum(q[:, o : o + 1] * new, axis=0, keepdims=True)
    readout = ro[...]
    gate = jnp.concatenate([rows[0][8:16], rows[1][8:16]], axis=0)
    hg = jnp.concatenate([head_gain[...], head_gain[...]], axis=0)
    readout = readout * lax.rsqrt(jnp.mean(readout * readout, axis=-1, keepdims=True) + RMS_EPS) * hg
    s_c[...] = (readout * (gate / (1.0 + jnp.exp(-gate)))).astype(BF16)

    slot_c = t * 16 + lax.rem(kv, 16)

    def send_c(src, slot, kv_to, t_to):
        pltpu.make_async_remote_copy(
            src_ref=src, dst_ref=r_c.at[slot], send_sem=c_send, recv_sem=c_recv.at[slot],
            device_id={"kv": kv_to, "tp": t_to}, device_id_type=MESH,
        ).start()

    for d, e in FAR:
        if e == 0 or d not in NEAR:
            send_c(s_c, slot_c, zd[d] * 4 + xd[e], half)

    @pl.when(jnp.logical_not(mine))
    def _():
        send_c(s_c, slot_c, kv, half)

    @pl.when(mine)
    def _():
        r_c[slot_c] = s_c[...]

    for d in NEAR:

        @pl.when(zd[d] // 4 == t)
        def _():
            for tt in range(2):
                slot = tt * 16 + (zd[d] - 4 * t) * 4 + xx
                drain(s_c, c_recv.at[slot])
                for e in (2, 1, 3):
                    send_c(r_c.at[slot], slot, z * 4 + xd[e], t)

    drain(r_g.at[t, pl.ds(0, 31)], g_sem.at[1])
    gains = rcopy(r_g.at[t], r_g.at[t], p_sem, kv, partner)
    gains.start()

    for d in range(8):
        for e in range(4):
            if e == 0 and d in NEAR:
                continue

            @pl.when(zd[d] // 4 == t)
            def _():
                for tt in range(2):
                    slot = tt * 16 + (zd[d] - 4 * t) * 4 + xd[e]
                    if d or e:
                        drain(s_c, c_recv.at[slot])
                    else:

                        @pl.when(t != tt)
                        def _():
                            drain(s_c, c_recv.at[slot])

    for tt in range(2):
        arrived = r_c[tt * 16 : (tt + 1) * 16].astype(F32).reshape(256, 256)
        for n in range(2):
            att32[n] = arrived[:, n * 128 : (n + 1) * 128]
            for h in range(8):
                at = tt * 2048 + h * 256 + n * 128
                att[:, at : at + 128] = att32[n, pl.ds(h, 32, stride=8), :].astype(BF16)
    wcopies[1].wait()
    mixed = jnp.concatenate([dot(att[...], owc[tt], NT) for tt in range(2)], axis=1)
    at_chip = pl.multiple_of(kv * 128, 128)
    res1 = ALPHA * x[:, pl.ds(at_chip, 128)].astype(F32) + mixed

    m_own = jnp.mean(res1, axis=-1, keepdims=True)
    sq[0:32, :] = jnp.broadcast_to(m_own, (32, 128))
    sq[32:128, :] = jnp.zeros((96, 128), F32)
    s_m[...] = sq[...].T[0:1, :]
    s_e[...] = (res1 - m_own).astype(BF16)

    def send_e(src, slot, kv_to):
        pltpu.make_async_remote_copy(
            src_ref=src, dst_ref=r_e.at[slot], send_sem=e_send, recv_sem=e_recv.at[slot],
            device_id={"kv": kv_to, "tp": t}, device_id_type=MESH,
        ).start()

    for d, e in FAR:
        if e == 0 or d not in NEAR:
            send_e(s_e, kv, zd[d] * 4 + xd[e])
    for d, e in FAR:
        rcopy(s_m, r_m.at[kv], m_sem, zd[d] * 4 + xd[e], t).start()
    for d in NEAR:
        slot = zd[d] * 4 + xx
        drain(s_e, e_recv.at[slot])
        for e in (2, 1, 3):
            send_e(r_e.at[slot], slot, z * 4 + xd[e])
    r_e[kv] = s_e[...]
    r_m[kv] = s_m[...]
    gains.wait()
    ga = r_g[0, :, 0, :]
    gb = r_g[1, :, 0, :]
    lane32 = iota((32, 128), 1) < 64
    gain1 = jnp.where(lane32, ga, pltpu.roll(gb, 64, 1))
    bias1 = jnp.where(lane32, pltpu.roll(ga, 64, 1), gb)
    wcopies[2].wait()
    wcopies[3].wait()
    drain(r_m.at[pl.ds(0, 31)], m_sem.at[1])
    for d, e in FAR:
        if e or d not in NEAR:
            drain(s_e, e_recv.at[zd[d] * 4 + xd[e]])
    sq[0:32, :] = r_m[:, 0, :]
    means = sq[...].T[0:32, 0:32]
    acc = jnp.zeros((32, 128), F32)
    for c in range(CHIPS):
        acc = acc + r_e[c].astype(F32)
    mean = (jnp.sum(acc, axis=-1, keepdims=True) + 128.0 * jnp.sum(means, axis=-1, keepdims=True)) / D
    acc = jnp.zeros((32, 128), F32)
    for c in range(CHIPS):
        v = r_e[c].astype(F32) + (means[:, c : c + 1] - mean)
        xt[c] = v
        acc = acc + v * v
    inv = lax.rsqrt(jnp.sum(acc, axis=-1, keepdims=True) / D + LN_EPS)
    for c in range(CHIPS):
        xn[:, c * 128 : (c + 1) * 128] = (xt[c] * inv * gain1[c : c + 1, :] + bias1[c : c + 1, :]).astype(BF16)

    hidden = []
    for tt in range(2):
        lifted = jnp.maximum(dot(xn[...], upc[tt], NN), 0.0)
        hidden.append((lifted * lifted).astype(BF16))
    for d in (4, 3, 5, 2, 6, 1, 7, 0):
        cl = pl.ds(pl.multiple_of(zd[d] * 512, 512), 512)
        y = (dot(hidden[0], dnc[0, :, cl], NN) + dot(hidden[1], dnc[1, :, cl], NN)).astype(BF16)
        for j in range(4):
            s_y[zd[d] * 4 + j] = y[:, j * 128 : (j + 1) * 128]
        for e in (2, 1, 3, 0):
            if d or e:
                kp = zd[d] * 4 + xd[e]
                rcopy(s_y.at[kp], r_y.at[kv], y_sem, kp, t).start()

    r_y[kv] = s_y[kv]
    drain(r_y.at[pl.ds(0, 31)], y_sem.at[1])
    res2 = ALPHA * xn[:, pl.ds(at_chip, 128)].astype(F32)
    for c in range(CHIPS):
        res2 = res2 + r_y[c].astype(F32)

    m_own = jnp.mean(res2, axis=-1, keepdims=True)
    dev = res2 - m_own
    v_own = jnp.sum(dev * dev, axis=-1, keepdims=True)
    sq[0:32, :] = jnp.where(iota((32, 128), 1) == 0, m_own, v_own)
    flat = sq[...].T
    s_h[...] = jnp.concatenate([flat[0:1, 0:32], flat[1:2, 0:32], flat[0:1, 0:64]], axis=1)
    s_f[...] = res2
    last = rcopy(s_f, r_f, f_sem, kv, partner)
    for d, e in FAR:
        for tt in range(2):
            rcopy(s_h, r_h.at[t * CHIPS + kv], h_sem, zd[d] * 4 + xd[e], tt).start()
    rcopy(s_h, r_h.at[t * CHIPS + kv], h_sem, kv, partner).start()
    last.start()
    r_h[t * CHIPS + kv] = s_h[...]
    own0 = r_g[0, kv][1:2, :]
    own1 = r_g[1, kv][1:2, :]
    lane1 = iota((1, 128), 1) < 64
    gain2 = jnp.where(lane1, own0, pltpu.roll(own1, 64, 1))
    bias2 = jnp.where(lane1, pltpu.roll(own0, 64, 1), own1)
    last.wait()
    drain(r_h.at[pl.ds(0, 63)], h_sem.at[1])
    for tt in range(2):
        ms = r_h[tt * CHIPS : (tt + 1) * CHIPS, 0, :]
        mean = jnp.mean(ms, axis=0, keepdims=True)
        dm = ms - mean
        first = jnp.sum(ms, axis=0, keepdims=True)
        spread = (first + pltpu.roll(128.0 * jnp.sum(dm * dm, axis=0, keepdims=True), 32, 1)) / D
        sq[2 * tt : 2 * tt + 1, :] = mean
        sq[2 * tt + 1 : 2 * tt + 2, :] = lax.rsqrt(spread + LN_EPS)
    back = sq[...].T
    for tt in range(2):
        rows2 = jnp.where(t == tt, res2, r_f[...])
        o = (rows2 - back[0:32, 2 * tt : 2 * tt + 1]) * back[32:64, 2 * tt + 1 : 2 * tt + 2] * gain2 + bias2
        out[32 * tt : 32 * tt + 32, :] = jnp.where(t == 0, o, pltpu.roll(o, 64, 1))[:, :64].astype(BF16)

    drain(r_a.at[pl.ds(0, 15)], az_send)
    drain(r_a.at[pl.ds(0, 48)], ax_send)
    drain(r_g.at[t, pl.ds(0, 31)], g_sem.at[0])
    sent = 3 + sum(1 if d in NEAR else 4 for d in range(1, 8))
    drain(r_c.at[pl.ds(0, sent)], c_send)

    @pl.when(mine)
    def _():
        drain(r_b.at[pl.ds(0, 31)], b_sem.at[0])

    @pl.when(jnp.logical_not(mine))
    def _():
        drain(r_b, b_sem.at[0])
        drain(s_c, c_send)

    for d in NEAR:

        @pl.when(zd[d] // 4 == t)
        def _():
            drain(r_c.at[pl.ds(0, 6)], c_send)

    drain(r_e.at[pl.ds(0, 31)], e_send)
    drain(r_m.at[pl.ds(0, 31)], m_sem.at[0])
    drain(r_y.at[pl.ds(0, 31)], y_sem.at[0])
    drain(r_h.at[pl.ds(0, 63)], h_sem.at[0])


def body(
    tokens, query_weight, key_weight, value_weight, gate_weight, decay_weight, decay_bias, states,
    head_gain, out_weight, norm1_gain, norm1_bias, up_weight, down_weight, norm2_gain, norm2_bias,
):
    flip = lambda w: w.transpose(1, 2, 0)
    flat = lambda w: flip(w).reshape(-1, D)
    line = lambda v: v.reshape(1, -1)
    vmem = pl.BlockSpec(memory_space=pltpu.VMEM)
    hbm = pl.BlockSpec(memory_space=pl.ANY)
    V = pltpu.VMEM
    dma = pltpu.SemaphoreType.DMA
    scratch = [
        V((64, 64), BF16), V((8, 128), F32), V((8, 256), F32),
        V((1, 64), F32), V((1, 64), F32), V((1, 64), F32), V((1, 64), F32),
        V((3, 8, 4, D), BF16),
        V((2, 224, D), BF16),
        V((2, 64, D), BF16),
        V((2, D, 256), BF16),
        V((2, 256, D), BF16),
        V((2, 8, 128, 256), F32),
        V((2, 16, 128), BF16), V((64, 16, 128), BF16),
        V((2, 128), F32), V((2, 32, 2, 128), F32),
        V((32, D), BF16),
        V((16, 2, 2, 256), F32), V((32, 2, 256), F32),
        V((16, 256), F32),
        V((16, 256), BF16), V((32, 16, 256), BF16),
        V((2, 256, 128), F32), V((32, D), BF16),
        V((32, 128), BF16), V((32, 32, 128), BF16),
        V((1, 128), F32), V((32, 1, 128), F32),
        V((32, 32, 128), F32), V((32, D), BF16),
        V((32, 32, 128), BF16), V((32, 32, 128), BF16),
        V((1, 128), F32), V((64, 1, 128), F32),
        V((32, 128), F32), V((32, 128), F32),
        V((128, 128), F32),
        dma((7,)), dma((9,)), dma((4,)), dma((4,)), dma, dma((16,)), dma, dma((8,)),
        dma((2,)), dma((2,)), dma((2,)), dma, dma((32,)), dma, dma((32,)),
    ] + [dma((2,))] * 4
    return pl.pallas_call(
        kernel,
        out_shape=(
            pltpu.VMEM((64, 64), BF16),
            pltpu.VMEM((2, 8, 128, 256), F32),
        ),
        in_specs=[hbm] * 16,
        out_specs=(vmem, vmem),
        scratch_shapes=scratch,
        compiler_params=pltpu.CompilerParams(
            collective_id=0, has_side_effects=True, vmem_limit_bytes=60 * 1024 * 1024
        ),
        name="layer_step",
    )(
        tokens, flip(query_weight), flip(key_weight), flip(decay_weight), flat(value_weight), flat(gate_weight),
        decay_bias, states, head_gain, out_weight.T, line(norm1_gain), line(norm1_bias), up_weight, down_weight,
        line(norm2_gain), line(norm2_bias),
    )


def solution(mesh):
    placed = (
        P("dp", ("kv", "tp")),
        P(None, "tp", "kv"),
        P(None, "tp", "kv"),
        P(None, "tp", "kv"),
        P(None, "tp", "kv"),
        P(None, "tp", "kv"),
        P("tp", None),
        P(("dp", "kv"), "tp", None, None),
        P("tp", None),
        P(None, ("kv", "tp")),
        P(("kv", "tp")),
        P(("kv", "tp")),
        P(None, ("kv", "tp")),
        P(("kv", "tp"), None),
        P(("kv", "tp")),
        P(("kv", "tp")),
    )
    return jax.shard_map(
        body,
        mesh=mesh,
        in_specs=placed,
        out_specs=(P("dp", ("kv", "tp")), P(("dp", "kv"), "tp", None, None)),
        check_vma=False,
    )
```

```python
import functools

import jax
import jax.numpy as jnp
from jax import lax
from jax.experimental import pallas as pl
from jax.experimental.pallas import tpu as pltpu
from jax.sharding import PartitionSpec as P

D = 4096
KEY_DIM = 128
ALPHA = 2.0**0.5
TAU = 16.0
LN_EPS = 1e-05
RMS_EPS = 1e-06
MESH = pl.DeviceIdType.MESH
F32 = jnp.float32
BF16 = jnp.bfloat16
NT = (((1,), (1,)), ((), ()))
NN = (((1,), (0,)), ((), ()))
TN = (((0,), (0,)), ((), ()))
CHIPS = 32
FAR = sorted(
    ((d, e) for d in range(8) for e in range(4) if d or e),
    key=lambda o: (-min(o[0], 8 - o[0]) - min(o[1], 4 - o[1]), o),
)
NEAR = (1, 7, 2, 6, 3, 5, 4)


def dot(a, b, dims):
    return lax.dot_general(a, b, dims, preferred_element_type=F32)


def iota(shape, dim):
    return lax.broadcasted_iota(jnp.int32, shape, dim)


def kernel(
    tok_h, wq, wk, wd, wv, wg, bias_h, states, head_gain_h, ow, g1_h, b1_h, up, dn, g2_h, b2_h,
    out, new_states,
    tok, bias, head_gain, g1, b1, g2, b2, wst, wc, owc, upc, dnc, st,
    s_a, r_a, s_g, r_g, x, s_b, r_b, ro, s_c, r_c, att32, att,
    s_e, r_e, s_m, r_m, xt, xn, s_y, r_y, s_h, r_h, s_f, r_f, sq,
    small_sem, own_sem, w_send, w_recv,
    az_send, az_recv, ax_send, ax_recv, g_sem, p_sem, b_sem, c_send, c_recv, e_send, e_recv, m_sem, y_sem, h_sem, f_sem,
):
    kv = lax.axis_index("kv")
    t = lax.axis_index("tp")
    z, xx = kv // 4, kv % 4
    half = kv // 16
    mine = half == t
    partner = 1 - t

    def wrap(v, n):
        return jnp.where(v >= n, v - n, v)

    zd = [wrap(z + d, 8) for d in range(8)]
    xd = [wrap(xx + d, 4) for d in range(4)]

    def rcopy(src, dst, sems, kv_to, t_to):
        return pltpu.make_async_remote_copy(
            src_ref=src, dst_ref=dst, send_sem=sems.at[0], recv_sem=sems.at[1],
            device_id={"kv": kv_to, "tp": t_to}, device_id_type=MESH,
        )

    def drain(ref, sem):
        pltpu.make_async_copy(ref, ref, sem).wait()

    barrier = pltpu.get_barrier_semaphore()

    def hello(kv_to, t_to):
        pl.semaphore_signal(barrier, inc=1, device_id={"kv": kv_to, "tp": t_to}, device_id_type=MESH)

    for d in (4, 3, 5, 2, 6, 1, 7):
        hello(zd[d] * 4 + xx, t)
        hello(zd[d] * 4 + xx, partner)
    for d in (2, 1, 3):
        hello(z * 4 + xd[d], t)
    hello(kv, partner)

    small = [
        pltpu.make_async_copy(a, b, small_sem.at[i])
        for i, (a, b) in enumerate(
            [(tok_h, tok), (bias_h, bias), (head_gain_h, head_gain), (g1_h, g1), (b1_h, b1), (g2_h, g2), (b2_h, b2)]
        )
    ]
    for c in small:
        c.start()

    own = [
        pltpu.make_async_copy(wq, wst.at[0], own_sem.at[0]),
        pltpu.make_async_copy(wk, wst.at[1], own_sem.at[1]),
        pltpu.make_async_copy(wd, wst.at[2], own_sem.at[2]),
        pltpu.make_async_copy(wv, wc.at[t, pl.ds(96, 64)], own_sem.at[3]),
        pltpu.make_async_copy(wg, wc.at[t, pl.ds(160, 64)], own_sem.at[4]),
        pltpu.make_async_copy(states, st, own_sem.at[5]),
        pltpu.make_async_copy(ow, owc.at[t], own_sem.at[6]),
        pltpu.make_async_copy(up, upc.at[t], own_sem.at[7]),
        pltpu.make_async_copy(dn, dnc.at[t], own_sem.at[8]),
    ]
    for c in own:
        c.start()

    for c in small:
        c.wait()
    tk = tok[...].astype(F32)
    for hh in range(2):
        s_a[hh] = jnp.concatenate(
            [tk[32 * hh : 32 * hh + 16], tk[32 * hh + 16 : 32 * hh + 32]], axis=1
        ).astype(BF16)
    s_g[0:1] = jnp.concatenate([g1[...], b1[...]], axis=1)
    s_g[1:2] = jnp.concatenate([g2[...], b2[...]], axis=1)
    me = kv * 2 + t
    r_a[me] = s_a[t]
    r_g[t, kv] = s_g[...]

    lane = iota((16, 128), 1) < 64
    col = iota((224, 256), 1)
    row = iota((224, 256), 0)
    low = col < 128
    j2 = col - 128
    src_low = ((col % 32) // 8) * 32 + (col % 8) * 4 + col // 32
    src_high = 96 + ((j2 % 16) // 8) * 64 + (j2 % 8) * 8 + j2 // 16
    src_low = jnp.where(col % 32 < 24, src_low, -1)
    perm = jnp.where(row == jnp.where(low, src_low, src_high), 1.0, 0.0).astype(BF16)
    e1 = jnp.where(iota((128, 128), 1) == (iota((128, 128), 0) % 4) * 32 + iota((128, 128), 0) // 4, 1.0, 0.0).astype(BF16)
    e2 = jnp.where(iota((256, 256), 0) == (iota((256, 256), 1) % 8) * 32 + iota((256, 256), 1) // 8, 1.0, 0.0).astype(BF16)
    zero = lambda n: jnp.zeros((n, 128), F32)
    bias_full = jnp.concatenate(
        [zero(16), bias[...], zero(24), bias[...], zero(8 + 64)], axis=0
    ).T[:, :64]

    for c in own[:5]:
        c.wait()
    for ty in range(3):
        for h in range(0, 8, 4):
            wc[t, ty * 32 + h * 4 : ty * 32 + h * 4 + 16, :] = jnp.concatenate(
                [wst[ty, h + i].astype(F32) for i in range(4)], axis=0
            ).astype(BF16)

    def wcopy(ref, i):
        return pltpu.make_async_remote_copy(
            src_ref=ref.at[t], dst_ref=ref.at[t], send_sem=w_send.at[i], recv_sem=w_recv.at[i],
            device_id={"kv": kv, "tp": partner}, device_id_type=MESH,
        )

    wcopies = [wcopy(wc, 0), wcopy(owc, 1), wcopy(upc, 2), wcopy(dnc, 3)]
    pl.semaphore_wait(barrier, 18)

    def to_line(src, kv_to, t_to):
        pltpu.make_async_remote_copy(
            src_ref=src, dst_ref=r_a.at[me], send_sem=az_send, recv_sem=az_recv.at[z * 2 + t],
            device_id={"kv": kv_to, "tp": t_to}, device_id_type=MESH,
        ).start()

    to_line(s_a.at[partner], kv, partner)
    for d in (4, 3, 5, 2, 6, 1, 7):
        for tt in range(2):
            to_line(s_a.at[tt], zd[d] * 4 + xx, tt)
    wcopies[0].start()
    for d in (0, 1, 7, 2, 6, 3, 5, 4):
        if d == 0:
            drain(r_a.at[0], az_recv.at[z * 2 + partner])
        else:
            drain(r_a.at[0], az_recv.at[zd[d] * 2])
            drain(r_a.at[0], az_recv.at[zd[d] * 2 + 1])
        block = r_a.at[pl.ds((zd[d] * 4 + xx) * 2, 2)]
        for e in (2, 1, 3):
            pltpu.make_async_remote_copy(
                src_ref=block, dst_ref=block, send_sem=ax_send, recv_sem=ax_recv.at[zd[d]],
                device_id={"kv": z * 4 + xd[e], "tp": t}, device_id_type=MESH,
            ).start()

    wcopies[0].wait()
    projected = [jnp.zeros((32, 224), F32) for _ in range(2)]
    for d in (0, 1, 7, 2, 6, 3, 5, 4):
        drain(r_a.at[pl.ds(0, 6)], ax_recv.at[zd[d]])
        tiles = []
        for j in range(4):
            a0 = r_a[zd[d] * 8 + 2 * j].astype(F32)
            a1 = r_a[zd[d] * 8 + 2 * j + 1].astype(F32)
            low = jnp.where(lane, a0, pltpu.roll(a1, 64, 1))
            high = jnp.where(lane, pltpu.roll(a0, 64, 1), a1)
            tiles.append(jnp.concatenate([low, high], axis=0).astype(BF16))
        tile = jnp.concatenate(tiles, axis=1)
        cl = pl.ds(pl.multiple_of(zd[d] * 512, 512), 512)
        x[:, cl] = tile
        for tt in range(2):
            projected[tt] = projected[tt] + dot(tile, wc[tt, :, cl], NT)
    for tt in range(2):
        p = projected[tt].astype(BF16)
        p = dot(p, perm, NN)
        for i in range(16):
            s_b[i, tt] = p[2 * i : 2 * i + 2, :]

    for i in range(4):
        zl = wrap(z - 4 * half + i, 4)
        for j in (2, 1, 3, 0):
            k16 = zl * 4 + xd[j]
            kp = 16 * t + k16
            for tt in range(2):
                if i == 0 and j == 0:

                    @pl.when(jnp.logical_not(jnp.logical_and(mine, t == tt)))
                    def _():
                        rcopy(s_b.at[k16, tt], r_b.at[kv], b_sem, kp, tt).start()

                else:
                    rcopy(s_b.at[k16, tt], r_b.at[kv], b_sem, kp, tt).start()

    for i in range(1, 4):
        own[5 + i].wait()
        wcopies[i].start()
    for d, e in FAR:
        rcopy(s_g, r_g.at[t, kv], g_sem, zd[d] * 4 + xd[e], t).start()
    own[5].wait()

    @pl.when(mine)
    def _():
        r_b[kv] = s_b[lax.rem(kv, 16), t]
        drain(r_b.at[pl.ds(0, 31)], b_sem.at[1])

    @pl.when(jnp.logical_not(mine))
    def _():
        drain(r_b, b_sem.at[1])

    qkd, vg = [], []
    for s in range(2):
        rs = r_b[:, s, :]
        qkd.append(jnp.concatenate([rs[:, c * 32 : (c + 1) * 32] for c in range(4)], axis=0))
        vg.append(jnp.concatenate([rs[:, 128 + c * 16 : 144 + c * 16] for c in range(8)], axis=0))
    cols = dot(e1, jnp.concatenate(qkd, axis=1).astype(BF16), NN)
    rows = [dot(v.astype(BF16), e2, TN) for v in vg]
    decay = cols + bias_full
    log_sig = jnp.minimum(decay, 0.0) - jnp.log1p(jnp.exp(-jnp.abs(decay)))
    retain = jnp.exp(log_sig / TAU)
    q = cols * KEY_DIM ** (-0.5)
    for s in range(2):
        for h in range(8):
            o = s * 32 + h
            new = retain[:, o + 16 : o + 17] * st[s, h] + cols[:, o + 8 : o + 9] * rows[s][h : h + 1, :]
            new_states[s, h] = new
            ro[s * 8 + h : s * 8 + h + 1, :] = jnp.sum(q[:, o : o + 1] * new, axis=0, keepdims=True)
    readout = ro[...]
    gate = jnp.concatenate([rows[0][8:16], rows[1][8:16]], axis=0)
    hg = jnp.concatenate([head_gain[...], head_gain[...]], axis=0)
    readout = readout * lax.rsqrt(jnp.mean(readout * readout, axis=-1, keepdims=True) + RMS_EPS) * hg
    s_c[...] = (readout * (gate / (1.0 + jnp.exp(-gate)))).astype(BF16)

    slot_c = t * 16 + lax.rem(kv, 16)

    def send_c(src, slot, kv_to, t_to):
        pltpu.make_async_remote_copy(
            src_ref=src, dst_ref=r_c.at[slot], send_sem=c_send, recv_sem=c_recv.at[slot],
            device_id={"kv": kv_to, "tp": t_to}, device_id_type=MESH,
        ).start()

    for d, e in FAR:
        if e == 0 or d not in NEAR:
            send_c(s_c, slot_c, zd[d] * 4 + xd[e], half)

    @pl.when(jnp.logical_not(mine))
    def _():
        send_c(s_c, slot_c, kv, half)

    @pl.when(mine)
    def _():
        r_c[slot_c] = s_c[...]

    for d in NEAR:

        @pl.when(zd[d] // 4 == t)
        def _():
            for tt in range(2):
                slot = tt * 16 + (zd[d] - 4 * t) * 4 + xx
                drain(s_c, c_recv.at[slot])
                for e in (2, 1, 3):
                    send_c(r_c.at[slot], slot, z * 4 + xd[e], t)

    drain(r_g.at[t, pl.ds(0, 31)], g_sem.at[1])
    gains = rcopy(r_g.at[t], r_g.at[t], p_sem, kv, partner)
    gains.start()

    for d in range(8):
        for e in range(4):
            if e == 0 and d in NEAR:
                continue

            @pl.when(zd[d] // 4 == t)
            def _():
                for tt in range(2):
                    slot = tt * 16 + (zd[d] - 4 * t) * 4 + xd[e]
                    if d or e:
                        drain(s_c, c_recv.at[slot])
                    else:

                        @pl.when(t != tt)
                        def _():
                            drain(s_c, c_recv.at[slot])

    for tt in range(2):
        arrived = r_c[tt * 16 : (tt + 1) * 16].astype(F32).reshape(256, 256)
        for n in range(2):
            att32[n] = arrived[:, n * 128 : (n + 1) * 128]
            for h in range(8):
                at = tt * 2048 + h * 256 + n * 128
                att[:, at : at + 128] = att32[n, pl.ds(h, 32, stride=8), :].astype(BF16)
    wcopies[1].wait()
    mixed = jnp.concatenate([dot(att[...], owc[tt], NT) for tt in range(2)], axis=1)
    at_chip = pl.multiple_of(kv * 128, 128)
    res1 = ALPHA * x[:, pl.ds(at_chip, 128)].astype(F32) + mixed

    m_own = jnp.mean(res1, axis=-1, keepdims=True)
    sq[0:32, :] = jnp.broadcast_to(m_own, (32, 128))
    sq[32:128, :] = jnp.zeros((96, 128), F32)
    s_m[...] = sq[...].T[0:1, :]
    s_e[...] = (res1 - m_own).astype(BF16)

    def send_e(src, slot, kv_to):
        pltpu.make_async_remote_copy(
            src_ref=src, dst_ref=r_e.at[slot], send_sem=e_send, recv_sem=e_recv.at[slot],
            device_id={"kv": kv_to, "tp": t}, device_id_type=MESH,
        ).start()

    for d, e in FAR:
        if e == 0 or d not in NEAR:
            send_e(s_e, kv, zd[d] * 4 + xd[e])
    for d, e in FAR:
        rcopy(s_m, r_m.at[kv], m_sem, zd[d] * 4 + xd[e], t).start()
    for d in NEAR:
        slot = zd[d] * 4 + xx
        drain(s_e, e_recv.at[slot])
        for e in (2, 1, 3):
            send_e(r_e.at[slot], slot, z * 4 + xd[e])
    r_e[kv] = s_e[...]
    r_m[kv] = s_m[...]
    gains.wait()
    ga = r_g[0, :, 0, :]
    gb = r_g[1, :, 0, :]
    lane32 = iota((32, 128), 1) < 64
    gain1 = jnp.where(lane32, ga, pltpu.roll(gb, 64, 1))
    bias1 = jnp.where(lane32, pltpu.roll(ga, 64, 1), gb)
    wcopies[2].wait()
    wcopies[3].wait()
    drain(r_m.at[pl.ds(0, 31)], m_sem.at[1])
    for d, e in FAR:
        if e or d not in NEAR:
            drain(s_e, e_recv.at[zd[d] * 4 + xd[e]])
    sq[0:32, :] = r_m[:, 0, :]
    means = sq[...].T[0:32, 0:32]
    acc = jnp.zeros((32, 128), F32)
    for c in range(CHIPS):
        acc = acc + r_e[c].astype(F32)
    mean = (jnp.sum(acc, axis=-1, keepdims=True) + 128.0 * jnp.sum(means, axis=-1, keepdims=True)) / D
    acc = jnp.zeros((32, 128), F32)
    for c in range(CHIPS):
        v = r_e[c].astype(F32) + (means[:, c : c + 1] - mean)
        xt[c] = v
        acc = acc + v * v
    inv = lax.rsqrt(jnp.sum(acc, axis=-1, keepdims=True) / D + LN_EPS)
    for c in range(CHIPS):
        xn[:, c * 128 : (c + 1) * 128] = (xt[c] * inv * gain1[c : c + 1, :] + bias1[c : c + 1, :]).astype(BF16)

    hidden = []
    for tt in range(2):
        lifted = jnp.maximum(dot(xn[...], upc[tt], NN), 0.0)
        hidden.append((lifted * lifted).astype(BF16))
    for d in (4, 3, 5, 2, 6, 1, 7, 0):
        cl = pl.ds(pl.multiple_of(zd[d] * 512, 512), 512)
        y = (dot(hidden[0], dnc[0, :, cl], NN) + dot(hidden[1], dnc[1, :, cl], NN)).astype(BF16)
        for j in range(4):
            s_y[zd[d] * 4 + j] = y[:, j * 128 : (j + 1) * 128]
        for e in (2, 1, 3, 0):
            if d or e:
                kp = zd[d] * 4 + xd[e]
                rcopy(s_y.at[kp], r_y.at[kv], y_sem, kp, t).start()

    r_y[kv] = s_y[kv]
    drain(r_y.at[pl.ds(0, 31)], y_sem.at[1])
    res2 = ALPHA * xn[:, pl.ds(at_chip, 128)].astype(F32)
    for c in range(CHIPS):
        res2 = res2 + r_y[c].astype(F32)

    m_own = jnp.mean(res2, axis=-1, keepdims=True)
    dev = res2 - m_own
    v_own = jnp.sum(dev * dev, axis=-1, keepdims=True)
    sq[0:32, :] = jnp.where(iota((32, 128), 1) == 0, m_own, v_own)
    flat = sq[...].T
    s_h[...] = jnp.concatenate([flat[0:1, 0:32], flat[1:2, 0:32], flat[0:1, 0:64]], axis=1)
    s_f[...] = res2
    last = rcopy(s_f, r_f, f_sem, kv, partner)
    for d, e in FAR:
        for tt in range(2):
            rcopy(s_h, r_h.at[t * CHIPS + kv], h_sem, zd[d] * 4 + xd[e], tt).start()
    rcopy(s_h, r_h.at[t * CHIPS + kv], h_sem, kv, partner).start()
    last.start()
    r_h[t * CHIPS + kv] = s_h[...]
    own0 = r_g[0, kv][1:2, :]
    own1 = r_g[1, kv][1:2, :]
    lane1 = iota((1, 128), 1) < 64
    gain2 = jnp.where(lane1, own0, pltpu.roll(own1, 64, 1))
    bias2 = jnp.where(lane1, pltpu.roll(own0, 64, 1), own1)
    last.wait()
    drain(r_h.at[pl.ds(0, 63)], h_sem.at[1])
    for tt in range(2):
        ms = r_h[tt * CHIPS : (tt + 1) * CHIPS, 0, :]
        mean = jnp.mean(ms, axis=0, keepdims=True)
        dm = ms - mean
        first = jnp.sum(ms, axis=0, keepdims=True)
        spread = (first + pltpu.roll(128.0 * jnp.sum(dm * dm, axis=0, keepdims=True), 32, 1)) / D
        sq[2 * tt : 2 * tt + 1, :] = mean
        sq[2 * tt + 1 : 2 * tt + 2, :] = lax.rsqrt(spread + LN_EPS)
    back = sq[...].T
    for tt in range(2):
        rows2 = jnp.where(t == tt, res2, r_f[...])
        o = (rows2 - back[0:32, 2 * tt : 2 * tt + 1]) * back[32:64, 2 * tt + 1 : 2 * tt + 2] * gain2 + bias2
        out[32 * tt : 32 * tt + 32, :] = jnp.where(t == 0, o, pltpu.roll(o, 64, 1))[:, :64].astype(BF16)

    drain(r_a.at[pl.ds(0, 15)], az_send)
    drain(r_a.at[pl.ds(0, 48)], ax_send)
    drain(r_g.at[t, pl.ds(0, 31)], g_sem.at[0])
    sent = 3 + sum(1 if d in NEAR else 4 for d in range(1, 8))
    drain(r_c.at[pl.ds(0, sent)], c_send)

    @pl.when(mine)
    def _():
        drain(r_b.at[pl.ds(0, 31)], b_sem.at[0])

    @pl.when(jnp.logical_not(mine))
    def _():
        drain(r_b, b_sem.at[0])
        drain(s_c, c_send)

    for d in NEAR:

        @pl.when(zd[d] // 4 == t)
        def _():
            drain(r_c.at[pl.ds(0, 6)], c_send)

    drain(r_e.at[pl.ds(0, 31)], e_send)
    drain(r_m.at[pl.ds(0, 31)], m_sem.at[0])
    drain(r_y.at[pl.ds(0, 31)], y_sem.at[0])
    drain(r_h.at[pl.ds(0, 63)], h_sem.at[0])


def body(
    tokens, query_weight, key_weight, value_weight, gate_weight, decay_weight, decay_bias, states,
    head_gain, out_weight, norm1_gain, norm1_bias, up_weight, down_weight, norm2_gain, norm2_bias,
):
    flip = lambda w: w.transpose(1, 2, 0)
    flat = lambda w: flip(w).reshape(-1, D)
    line = lambda v: v.reshape(1, -1)
    vmem = pl.BlockSpec(memory_space=pltpu.VMEM)
    hbm = pl.BlockSpec(memory_space=pl.ANY)
    V = pltpu.VMEM
    dma = pltpu.SemaphoreType.DMA
    scratch = [
        V((64, 64), BF16), V((8, 128), F32), V((8, 256), F32),
        V((1, 64), F32), V((1, 64), F32), V((1, 64), F32), V((1, 64), F32),
        V((3, 8, 4, D), BF16),
        V((2, 224, D), BF16),
        V((2, 64, D), BF16),
        V((2, D, 256), BF16),
        V((2, 256, D), BF16),
        V((2, 8, 128, 256), F32),
        V((2, 16, 128), BF16), V((64, 16, 128), BF16),
        V((2, 128), F32), V((2, 32, 2, 128), F32),
        V((32, D), BF16),
        V((16, 2, 2, 256), F32), V((32, 2, 256), F32),
        V((16, 256), F32),
        V((16, 256), BF16), V((32, 16, 256), BF16),
        V((2, 256, 128), F32), V((32, D), BF16),
        V((32, 128), BF16), V((32, 32, 128), BF16),
        V((1, 128), F32), V((32, 1, 128), F32),
        V((32, 32, 128), F32), V((32, D), BF16),
        V((32, 32, 128), BF16), V((32, 32, 128), BF16),
        V((1, 128), F32), V((64, 1, 128), F32),
        V((32, 128), F32), V((32, 128), F32),
        V((128, 128), F32),
        dma((7,)), dma((9,)), dma((4,)), dma((4,)), dma, dma((16,)), dma, dma((8,)),
        dma((2,)), dma((2,)), dma((2,)), dma, dma((32,)), dma, dma((32,)),
    ] + [dma((2,))] * 4
    return pl.pallas_call(
        kernel,
        out_shape=(
            pltpu.VMEM((64, 64), BF16),
            pltpu.VMEM((2, 8, 128, 256), F32),
        ),
        in_specs=[hbm] * 16,
        out_specs=(vmem, vmem),
        scratch_shapes=scratch,
        compiler_params=pltpu.CompilerParams(
            collective_id=0, has_side_effects=True, vmem_limit_bytes=60 * 1024 * 1024
        ),
        name="layer_step",
    )(
        tokens, flip(query_weight), flip(key_weight), flip(decay_weight), flat(value_weight), flat(gate_weight),
        decay_bias, states, head_gain, out_weight.T, line(norm1_gain), line(norm1_bias), up_weight, down_weight,
        line(norm2_gain), line(norm2_bias),
    )


def solution(mesh):
    placed = (
        P("dp", ("kv", "tp")),
        P(None, "tp", "kv"),
        P(None, "tp", "kv"),
        P(None, "tp", "kv"),
        P(None, "tp", "kv"),
        P(None, "tp", "kv"),
        P("tp", None),
        P(("dp", "kv"), "tp", None, None),
        P("tp", None),
        P(None, ("kv", "tp")),
        P(("kv", "tp")),
        P(("kv", "tp")),
        P(None, ("kv", "tp")),
        P(("kv", "tp"), None),
        P(("kv", "tp")),
        P(("kv", "tp")),
    )
    return jax.shard_map(
        body,
        mesh=mesh,
        in_specs=placed,
        out_specs=(P("dp", ("kv", "tp")), P(("dp", "kv"), "tp", None, None)),
        check_vma=False,
    )
```

```python
import functools

import jax
import jax.numpy as jnp
from jax import lax
from jax.experimental import pallas as pl
from jax.experimental.pallas import tpu as pltpu
from jax.sharding import PartitionSpec as P

D = 4096
KEY_DIM = 128
ALPHA = 2.0**0.5
TAU = 16.0
LN_EPS = 1e-05
RMS_EPS = 1e-06
MESH = pl.DeviceIdType.MESH
F32 = jnp.float32
BF16 = jnp.bfloat16
NT = (((1,), (1,)), ((), ()))
NN = (((1,), (0,)), ((), ()))
TN = (((0,), (0,)), ((), ()))
CHIPS = 32
FAR = sorted(
    ((d, e) for d in range(8) for e in range(4) if d or e),
    key=lambda o: (-min(o[0], 8 - o[0]) - min(o[1], 4 - o[1]), o),
)
NEAR = (1, 7, 2, 6, 3, 5, 4)


def dot(a, b, dims):
    return lax.dot_general(a, b, dims, preferred_element_type=F32)


def iota(shape, dim):
    return lax.broadcasted_iota(jnp.int32, shape, dim)


def kernel(
    tok_h, wq, wk, wd, wv, wg, bias_h, states, head_gain_h, ow, g1_h, b1_h, up, dn, g2_h, b2_h,
    out, new_states,
    tok, bias, head_gain, g1, b1, g2, b2, wst, wc, owc, upc, dnc, st,
    s_a, r_a, s_g, r_g, x, s_b, r_b, ro, s_c, r_c, att32, att,
    s_e, r_e, s_m, r_m, gain1, bias1, gm, s_y, r_y, s_h, r_h, s_f, r_f, sq,
    small_sem, own_sem, w_send, w_recv,
    az_send, az_recv, ax_send, ax_recv, g_sem, p_sem, b_sem, c_send, c_recv, e_send, e_recv, m_sem, y_sem, h_sem, f_sem,
):
    kv = lax.axis_index("kv")
    t = lax.axis_index("tp")
    z, xx = kv // 4, kv % 4
    half = kv // 16
    mine = half == t
    partner = 1 - t

    def wrap(v, n):
        return jnp.where(v >= n, v - n, v)

    zd = [wrap(z + d, 8) for d in range(8)]
    xd = [wrap(xx + d, 4) for d in range(4)]

    def rcopy(src, dst, sems, kv_to, t_to):
        return pltpu.make_async_remote_copy(
            src_ref=src, dst_ref=dst, send_sem=sems.at[0], recv_sem=sems.at[1],
            device_id={"kv": kv_to, "tp": t_to}, device_id_type=MESH,
        )

    def drain(ref, sem):
        pltpu.make_async_copy(ref, ref, sem).wait()

    barrier = pltpu.get_barrier_semaphore()

    def hello(kv_to, t_to):
        pl.semaphore_signal(barrier, inc=1, device_id={"kv": kv_to, "tp": t_to}, device_id_type=MESH)

    for d in (4, 3, 5, 2, 6, 1, 7):
        hello(zd[d] * 4 + xx, t)
        hello(zd[d] * 4 + xx, partner)
    for d in (2, 1, 3):
        hello(z * 4 + xd[d], t)
    hello(kv, partner)

    small = [
        pltpu.make_async_copy(a, b, small_sem.at[i])
        for i, (a, b) in enumerate(
            [(tok_h, tok), (bias_h, bias), (head_gain_h, head_gain), (g1_h, g1), (b1_h, b1), (g2_h, g2), (b2_h, b2)]
        )
    ]
    for c in small:
        c.start()

    own = [
        pltpu.make_async_copy(wq, wst.at[0], own_sem.at[0]),
        pltpu.make_async_copy(wk, wst.at[1], own_sem.at[1]),
        pltpu.make_async_copy(wd, wst.at[2], own_sem.at[2]),
        pltpu.make_async_copy(wv, wc.at[t, pl.ds(96, 64)], own_sem.at[3]),
        pltpu.make_async_copy(wg, wc.at[t, pl.ds(160, 64)], own_sem.at[4]),
        pltpu.make_async_copy(states, st, own_sem.at[5]),
        pltpu.make_async_copy(ow, owc.at[t], own_sem.at[6]),
        pltpu.make_async_copy(up, upc.at[t], own_sem.at[7]),
        pltpu.make_async_copy(dn, dnc.at[t], own_sem.at[8]),
    ]
    for c in own:
        c.start()

    for c in small:
        c.wait()
    tk = tok[...].astype(F32)
    for hh in range(2):
        s_a[hh] = jnp.concatenate(
            [tk[32 * hh : 32 * hh + 16], tk[32 * hh + 16 : 32 * hh + 32]], axis=1
        ).astype(BF16)
    s_g[0:1] = jnp.concatenate([g1[...], b1[...]], axis=1)
    s_g[1:2] = jnp.concatenate([g2[...], b2[...]], axis=1)
    me = kv * 2 + t
    r_a[me] = s_a[t]
    r_g[t, kv] = s_g[...]

    lane = iota((16, 128), 1) < 64
    col = iota((224, 256), 1)
    row = iota((224, 256), 0)
    low = col < 128
    j2 = col - 128
    src_low = ((col % 32) // 8) * 32 + (col % 8) * 4 + col // 32
    src_high = 96 + ((j2 % 16) // 8) * 64 + (j2 % 8) * 8 + j2 // 16
    src_low = jnp.where(col % 32 < 24, src_low, -1)
    perm = jnp.where(row == jnp.where(low, src_low, src_high), 1.0, 0.0).astype(BF16)
    e1 = jnp.where(iota((128, 128), 1) == (iota((128, 128), 0) % 4) * 32 + iota((128, 128), 0) // 4, 1.0, 0.0).astype(BF16)
    e2 = jnp.where(iota((256, 256), 0) == (iota((256, 256), 1) % 8) * 32 + iota((256, 256), 1) // 8, 1.0, 0.0).astype(BF16)
    zero = lambda n: jnp.zeros((n, 128), F32)
    bias_full = jnp.concatenate(
        [zero(16), bias[...], zero(24), bias[...], zero(8 + 64)], axis=0
    ).T[:, :64]

    for c in own[:5]:
        c.wait()
    for ty in range(3):
        for h in range(0, 8, 4):
            wc[t, ty * 32 + h * 4 : ty * 32 + h * 4 + 16, :] = jnp.concatenate(
                [wst[ty, h + i].astype(F32) for i in range(4)], axis=0
            ).astype(BF16)

    def wcopy(ref, i):
        return pltpu.make_async_remote_copy(
            src_ref=ref.at[t], dst_ref=ref.at[t], send_sem=w_send.at[i], recv_sem=w_recv.at[i],
            device_id={"kv": kv, "tp": partner}, device_id_type=MESH,
        )

    wcopies = [wcopy(wc, 0), wcopy(owc, 1), wcopy(upc, 2), wcopy(dnc, 3)]
    pl.semaphore_wait(barrier, 18)

    def to_line(src, kv_to, t_to):
        pltpu.make_async_remote_copy(
            src_ref=src, dst_ref=r_a.at[me], send_sem=az_send, recv_sem=az_recv.at[z * 2 + t],
            device_id={"kv": kv_to, "tp": t_to}, device_id_type=MESH,
        ).start()

    to_line(s_a.at[partner], kv, partner)
    for d in (4, 3, 5, 2, 6, 1, 7):
        for tt in range(2):
            to_line(s_a.at[tt], zd[d] * 4 + xx, tt)
    wcopies[0].start()
    for d in (0, 1, 7, 2, 6, 3, 5, 4):
        if d == 0:
            drain(r_a.at[0], az_recv.at[z * 2 + partner])
        else:
            drain(r_a.at[0], az_recv.at[zd[d] * 2])
            drain(r_a.at[0], az_recv.at[zd[d] * 2 + 1])
        block = r_a.at[pl.ds((zd[d] * 4 + xx) * 2, 2)]
        for e in (2, 1, 3):
            pltpu.make_async_remote_copy(
                src_ref=block, dst_ref=block, send_sem=ax_send, recv_sem=ax_recv.at[zd[d]],
                device_id={"kv": z * 4 + xd[e], "tp": t}, device_id_type=MESH,
            ).start()

    wcopies[0].wait()
    projected = [jnp.zeros((32, 224), F32) for _ in range(2)]
    for d in (0, 1, 7, 2, 6, 3, 5, 4):
        drain(r_a.at[pl.ds(0, 6)], ax_recv.at[zd[d]])
        tiles = []
        for j in range(4):
            a0 = r_a[zd[d] * 8 + 2 * j].astype(F32)
            a1 = r_a[zd[d] * 8 + 2 * j + 1].astype(F32)
            low = jnp.where(lane, a0, pltpu.roll(a1, 64, 1))
            high = jnp.where(lane, pltpu.roll(a0, 64, 1), a1)
            tiles.append(jnp.concatenate([low, high], axis=0).astype(BF16))
        tile = jnp.concatenate(tiles, axis=1)
        cl = pl.ds(pl.multiple_of(zd[d] * 512, 512), 512)
        x[:, cl] = tile
        for tt in range(2):
            projected[tt] = projected[tt] + dot(tile, wc[tt, :, cl], NT)
    for tt in range(2):
        p = projected[tt].astype(BF16)
        p = dot(p, perm, NN)
        for i in range(16):
            s_b[i, tt] = p[2 * i : 2 * i + 2, :]

    for i in range(4):
        zl = wrap(z - 4 * half + i, 4)
        for j in (2, 1, 3, 0):
            k16 = zl * 4 + xd[j]
            kp = 16 * t + k16
            for tt in range(2):
                if i == 0 and j == 0:

                    @pl.when(jnp.logical_not(jnp.logical_and(mine, t == tt)))
                    def _():
                        rcopy(s_b.at[k16, tt], r_b.at[kv], b_sem, kp, tt).start()

                else:
                    rcopy(s_b.at[k16, tt], r_b.at[kv], b_sem, kp, tt).start()

    for i in range(1, 4):
        own[5 + i].wait()
        wcopies[i].start()
    for d, e in FAR:
        rcopy(s_g, r_g.at[t, kv], g_sem, zd[d] * 4 + xd[e], t).start()
    own[5].wait()

    @pl.when(mine)
    def _():
        r_b[kv] = s_b[lax.rem(kv, 16), t]
        drain(r_b.at[pl.ds(0, 31)], b_sem.at[1])

    @pl.when(jnp.logical_not(mine))
    def _():
        drain(r_b, b_sem.at[1])

    qkd, vg = [], []
    for s in range(2):
        rs = r_b[:, s, :]
        qkd.append(jnp.concatenate([rs[:, c * 32 : (c + 1) * 32] for c in range(4)], axis=0))
        vg.append(jnp.concatenate([rs[:, 128 + c * 16 : 144 + c * 16] for c in range(8)], axis=0))
    cols = dot(e1, jnp.concatenate(qkd, axis=1).astype(BF16), NN)
    rows = [dot(v.astype(BF16), e2, TN) for v in vg]
    decay = cols + bias_full
    log_sig = jnp.minimum(decay, 0.0) - jnp.log1p(jnp.exp(-jnp.abs(decay)))
    retain = jnp.exp(log_sig / TAU)
    q = cols * KEY_DIM ** (-0.5)
    for s in range(2):
        for h in range(8):
            o = s * 32 + h
            new = retain[:, o + 16 : o + 17] * st[s, h] + cols[:, o + 8 : o + 9] * rows[s][h : h + 1, :]
            new_states[s, h] = new
            ro[s * 8 + h : s * 8 + h + 1, :] = jnp.sum(q[:, o : o + 1] * new, axis=0, keepdims=True)
    readout = ro[...]
    gate = jnp.concatenate([rows[0][8:16], rows[1][8:16]], axis=0)
    hg = jnp.concatenate([head_gain[...], head_gain[...]], axis=0)
    readout = readout * lax.rsqrt(jnp.mean(readout * readout, axis=-1, keepdims=True) + RMS_EPS) * hg
    s_c[...] = (readout * (gate / (1.0 + jnp.exp(-gate)))).astype(BF16)

    slot_c = t * 16 + lax.rem(kv, 16)

    drain(r_g.at[t, pl.ds(0, 31)], g_sem.at[1])
    gains = rcopy(r_g.at[t], r_g.at[t], p_sem, kv, partner)
    gains.start()

    def send_c(src, slot, kv_to, t_to):
        pltpu.make_async_remote_copy(
            src_ref=src, dst_ref=r_c.at[slot], send_sem=c_send, recv_sem=c_recv.at[slot],
            device_id={"kv": kv_to, "tp": t_to}, device_id_type=MESH,
        ).start()

    for d, e in FAR:
        if e == 0 or d not in NEAR:
            send_c(s_c, slot_c, zd[d] * 4 + xd[e], half)

    @pl.when(jnp.logical_not(mine))
    def _():
        send_c(s_c, slot_c, kv, half)

    @pl.when(mine)
    def _():
        r_c[slot_c] = s_c[...]

    for d in NEAR:

        @pl.when(zd[d] // 4 == t)
        def _():
            for tt in range(2):
                slot = tt * 16 + (zd[d] - 4 * t) * 4 + xx
                drain(s_c, c_recv.at[slot])
                for e in (2, 1, 3):
                    send_c(r_c.at[slot], slot, z * 4 + xd[e], t)

    gains.wait()
    ga = r_g[0, :, 0, :]
    gb = r_g[1, :, 0, :]
    lane32 = iota((32, 128), 1) < 64
    gain1[...] = jnp.where(lane32, ga, pltpu.roll(gb, 64, 1))
    bias1[...] = jnp.where(lane32, pltpu.roll(ga, 64, 1), gb)
    wcopies[2].wait()
    shift = [jnp.zeros((1, 256), F32) for _ in range(2)]
    for c in range(CHIPS):
        parts = []
        for v in (gain1[c : c + 1, :], bias1[c : c + 1, :]):
            high = v.astype(BF16).astype(F32)
            parts += [high, v - high]
        parts = jnp.concatenate(parts + [jnp.zeros((4, 128), F32)], axis=0).astype(BF16)
        for tt in range(2):
            r = dot(parts, upc[tt, c * 128 : (c + 1) * 128, :], NN)
            gm[tt, c : c + 1, :] = r[0:1] + r[1:2]
            shift[tt] = shift[tt] + (r[2:3] + r[3:4])

    for d in range(8):
        for e in range(4):
            if e == 0 and d in NEAR:
                continue

            @pl.when(zd[d] // 4 == t)
            def _():
                for tt in range(2):
                    slot = tt * 16 + (zd[d] - 4 * t) * 4 + xd[e]
                    if d or e:
                        drain(s_c, c_recv.at[slot])
                    else:

                        @pl.when(t != tt)
                        def _():
                            drain(s_c, c_recv.at[slot])

    for tt in range(2):
        arrived = r_c[tt * 16 : (tt + 1) * 16].astype(F32).reshape(256, 256)
        for n in range(2):
            att32[n] = arrived[:, n * 128 : (n + 1) * 128]
            for h in range(8):
                at = tt * 2048 + h * 256 + n * 128
                att[:, at : at + 128] = att32[n, pl.ds(h, 32, stride=8), :].astype(BF16)
    wcopies[1].wait()
    mixed = jnp.concatenate([dot(att[...], owc[tt], NT) for tt in range(2)], axis=1)
    at_chip = pl.multiple_of(kv * 128, 128)
    res1 = ALPHA * x[:, pl.ds(at_chip, 128)].astype(F32) + mixed

    m_own = jnp.mean(res1, axis=-1, keepdims=True)
    sq[0:32, :] = jnp.broadcast_to(m_own, (32, 128))
    sq[32:128, :] = jnp.zeros((96, 128), F32)
    s_m[...] = sq[...].T[0:1, :]
    s_e[...] = (res1 - m_own).astype(BF16)

    def send_e(src, slot, kv_to):
        pltpu.make_async_remote_copy(
            src_ref=src, dst_ref=r_e.at[slot], send_sem=e_send, recv_sem=e_recv.at[slot],
            device_id={"kv": kv_to, "tp": t}, device_id_type=MESH,
        ).start()

    for d, e in FAR:
        if e == 0 or d not in NEAR:
            send_e(s_e, kv, zd[d] * 4 + xd[e])
    for d, e in FAR:
        rcopy(s_m, r_m.at[kv], m_sem, zd[d] * 4 + xd[e], t).start()
    for d in NEAR:
        slot = zd[d] * 4 + xx
        drain(s_e, e_recv.at[slot])
        for e in (2, 1, 3):
            send_e(r_e.at[slot], slot, z * 4 + xd[e])
    r_e[kv] = s_e[...]
    r_m[kv] = s_m[...]
    raw = [jnp.zeros((32, 256), F32) for _ in range(2)]
    acc = jnp.zeros((32, 128), F32)
    for d in (0, 1, 7, 2, 6, 3, 5, 4):
        tiles = []
        for e in range(1, 4):
            drain(s_e, e_recv.at[zd[d] * 4 + xd[e]])
        for j in range(4):
            v = r_e[zd[d] * 4 + j].astype(F32)
            acc = acc + v
            tiles.append((v * gain1[pl.ds(zd[d] * 4 + j, 1), :]).astype(BF16))
        tile = jnp.concatenate(tiles, axis=1)
        for tt in range(2):
            raw[tt] = raw[tt] + dot(tile, upc[tt, pl.ds(pl.multiple_of(zd[d] * 512, 512), 512), :], NN)
    drain(r_m.at[pl.ds(0, 31)], m_sem.at[1])
    sq[0:32, :] = r_m[:, 0, :]
    means = sq[...].T[0:32, 0:32]
    mean = (jnp.sum(acc, axis=-1, keepdims=True) + 128.0 * jnp.sum(means, axis=-1, keepdims=True)) / D
    means = means - mean
    acc = jnp.zeros((32, 128), F32)
    for c in range(CHIPS):
        v = r_e[c].astype(F32) + means[:, c : c + 1]
        acc = acc + v * v
    inv = lax.rsqrt(jnp.sum(acc, axis=-1, keepdims=True) / D + LN_EPS)
    own_gain = gain1[pl.ds(kv, 1), :]
    own_bias = bias1[pl.ds(kv, 1), :]
    normed = ((s_e[...].astype(F32) + (m_own - mean)) * inv * own_gain + own_bias).astype(BF16)

    wcopies[3].wait()
    hidden = []
    for tt in range(2):
        level = lax.dot_general(means, gm[tt], NN, precision=lax.Precision.HIGHEST, preferred_element_type=F32)
        lifted = jnp.maximum((raw[tt] + level) * inv + shift[tt], 0.0)
        hidden.append((lifted * lifted).astype(BF16))
    for d in (4, 3, 5, 2, 6, 1, 7, 0):
        cl = pl.ds(pl.multiple_of(zd[d] * 512, 512), 512)
        y = (dot(hidden[0], dnc[0, :, cl], NN) + dot(hidden[1], dnc[1, :, cl], NN)).astype(BF16)
        for j in range(4):
            s_y[zd[d] * 4 + j] = y[:, j * 128 : (j + 1) * 128]
        for e in (2, 1, 3, 0):
            if d or e:
                kp = zd[d] * 4 + xd[e]
                rcopy(s_y.at[kp], r_y.at[kv], y_sem, kp, t).start()

    r_y[kv] = s_y[kv]
    drain(r_y.at[pl.ds(0, 31)], y_sem.at[1])
    res2 = ALPHA * normed.astype(F32)
    for c in range(CHIPS):
        res2 = res2 + r_y[c].astype(F32)

    m_own = jnp.mean(res2, axis=-1, keepdims=True)
    dev = res2 - m_own
    v_own = jnp.sum(dev * dev, axis=-1, keepdims=True)
    sq[0:32, :] = jnp.where(iota((32, 128), 1) == 0, m_own, v_own)
    flat = sq[...].T
    s_h[...] = jnp.concatenate([flat[0:1, 0:32], flat[1:2, 0:32], flat[0:1, 0:64]], axis=1)
    s_f[...] = res2
    last = rcopy(s_f, r_f, f_sem, kv, partner)
    for d, e in FAR:
        for tt in range(2):
            rcopy(s_h, r_h.at[t * CHIPS + kv], h_sem, zd[d] * 4 + xd[e], tt).start()
    rcopy(s_h, r_h.at[t * CHIPS + kv], h_sem, kv, partner).start()
    last.start()
    r_h[t * CHIPS + kv] = s_h[...]
    own0 = r_g[0, kv][1:2, :]
    own1 = r_g[1, kv][1:2, :]
    lane1 = iota((1, 128), 1) < 64
    gain2 = jnp.where(lane1, own0, pltpu.roll(own1, 64, 1))
    bias2 = jnp.where(lane1, pltpu.roll(own0, 64, 1), own1)
    last.wait()
    drain(r_h.at[pl.ds(0, 63)], h_sem.at[1])
    for tt in range(2):
        ms = r_h[tt * CHIPS : (tt + 1) * CHIPS, 0, :]
        mean = jnp.mean(ms, axis=0, keepdims=True)
        dm = ms - mean
        first = jnp.sum(ms, axis=0, keepdims=True)
        spread = (first + pltpu.roll(128.0 * jnp.sum(dm * dm, axis=0, keepdims=True), 32, 1)) / D
        sq[2 * tt : 2 * tt + 1, :] = mean
        sq[2 * tt + 1 : 2 * tt + 2, :] = lax.rsqrt(spread + LN_EPS)
    back = sq[...].T
    for tt in range(2):
        rows2 = jnp.where(t == tt, res2, r_f[...])
        o = (rows2 - back[0:32, 2 * tt : 2 * tt + 1]) * back[32:64, 2 * tt + 1 : 2 * tt + 2] * gain2 + bias2
        out[32 * tt : 32 * tt + 32, :] = jnp.where(t == 0, o, pltpu.roll(o, 64, 1))[:, :64].astype(BF16)

    drain(r_a.at[pl.ds(0, 15)], az_send)
    drain(r_a.at[pl.ds(0, 48)], ax_send)
    drain(r_g.at[t, pl.ds(0, 31)], g_sem.at[0])
    sent = 3 + sum(1 if d in NEAR else 4 for d in range(1, 8))
    drain(r_c.at[pl.ds(0, sent)], c_send)

    @pl.when(mine)
    def _():
        drain(r_b.at[pl.ds(0, 31)], b_sem.at[0])

    @pl.when(jnp.logical_not(mine))
    def _():
        drain(r_b, b_sem.at[0])
        drain(s_c, c_send)

    for d in NEAR:

        @pl.when(zd[d] // 4 == t)
        def _():
            drain(r_c.at[pl.ds(0, 6)], c_send)

    drain(r_e.at[pl.ds(0, 31)], e_send)
    drain(r_m.at[pl.ds(0, 31)], m_sem.at[0])
    drain(r_y.at[pl.ds(0, 31)], y_sem.at[0])
    drain(r_h.at[pl.ds(0, 63)], h_sem.at[0])


def body(
    tokens, query_weight, key_weight, value_weight, gate_weight, decay_weight, decay_bias, states,
    head_gain, out_weight, norm1_gain, norm1_bias, up_weight, down_weight, norm2_gain, norm2_bias,
):
    flip = lambda w: w.transpose(1, 2, 0)
    flat = lambda w: flip(w).reshape(-1, D)
    line = lambda v: v.reshape(1, -1)
    vmem = pl.BlockSpec(memory_space=pltpu.VMEM)
    hbm = pl.BlockSpec(memory_space=pl.ANY)
    V = pltpu.VMEM
    dma = pltpu.SemaphoreType.DMA
    scratch = [
        V((64, 64), BF16), V((8, 128), F32), V((8, 256), F32),
        V((1, 64), F32), V((1, 64), F32), V((1, 64), F32), V((1, 64), F32),
        V((3, 8, 4, D), BF16),
        V((2, 224, D), BF16),
        V((2, 64, D), BF16),
        V((2, D, 256), BF16),
        V((2, 256, D), BF16),
        V((2, 8, 128, 256), F32),
        V((2, 16, 128), BF16), V((64, 16, 128), BF16),
        V((2, 128), F32), V((2, 32, 2, 128), F32),
        V((32, D), BF16),
        V((16, 2, 2, 256), F32), V((32, 2, 256), F32),
        V((16, 256), F32),
        V((16, 256), BF16), V((32, 16, 256), BF16),
        V((2, 256, 128), F32), V((32, D), BF16),
        V((32, 128), BF16), V((32, 32, 128), BF16),
        V((1, 128), F32), V((32, 1, 128), F32),
        V((32, 128), F32), V((32, 128), F32), V((2, 32, 256), F32),
        V((32, 32, 128), BF16), V((32, 32, 128), BF16),
        V((1, 128), F32), V((64, 1, 128), F32),
        V((32, 128), F32), V((32, 128), F32),
        V((128, 128), F32),
        dma((7,)), dma((9,)), dma((4,)), dma((4,)), dma, dma((16,)), dma, dma((8,)),
        dma((2,)), dma((2,)), dma((2,)), dma, dma((32,)), dma, dma((32,)),
    ] + [dma((2,))] * 4
    return pl.pallas_call(
        kernel,
        out_shape=(
            pltpu.VMEM((64, 64), BF16),
            pltpu.VMEM((2, 8, 128, 256), F32),
        ),
        in_specs=[hbm] * 16,
        out_specs=(vmem, vmem),
        scratch_shapes=scratch,
        compiler_params=pltpu.CompilerParams(
            collective_id=0, has_side_effects=True, vmem_limit_bytes=60 * 1024 * 1024
        ),
        name="layer_step",
    )(
        tokens, flip(query_weight), flip(key_weight), flip(decay_weight), flat(value_weight), flat(gate_weight),
        decay_bias, states, head_gain, out_weight.T, line(norm1_gain), line(norm1_bias), up_weight, down_weight,
        line(norm2_gain), line(norm2_bias),
    )


def solution(mesh):
    placed = (
        P("dp", ("kv", "tp")),
        P(None, "tp", "kv"),
        P(None, "tp", "kv"),
        P(None, "tp", "kv"),
        P(None, "tp", "kv"),
        P(None, "tp", "kv"),
        P("tp", None),
        P(("dp", "kv"), "tp", None, None),
        P("tp", None),
        P(None, ("kv", "tp")),
        P(("kv", "tp")),
        P(("kv", "tp")),
        P(None, ("kv", "tp")),
        P(("kv", "tp"), None),
        P(("kv", "tp")),
        P(("kv", "tp")),
    )
    return jax.shard_map(
        body,
        mesh=mesh,
        in_specs=placed,
        out_specs=(P("dp", ("kv", "tp")), P(("dp", "kv"), "tp", None, None)),
        check_vma=False,
    )
```

```python
import functools

import jax
import jax.numpy as jnp
from jax import lax
from jax.experimental import pallas as pl
from jax.experimental.pallas import tpu as pltpu
from jax.sharding import PartitionSpec as P

D = 4096
KEY_DIM = 128
ALPHA = 2.0**0.5
TAU = 16.0
LN_EPS = 1e-05
RMS_EPS = 1e-06
MESH = pl.DeviceIdType.MESH
F32 = jnp.float32
BF16 = jnp.bfloat16
NT = (((1,), (1,)), ((), ()))
NN = (((1,), (0,)), ((), ()))
TN = (((0,), (0,)), ((), ()))
CHIPS = 32
FAR = sorted(
    ((d, e) for d in range(8) for e in range(4) if d or e),
    key=lambda o: (-min(o[0], 8 - o[0]) - min(o[1], 4 - o[1]), o),
)
NEAR = (1, 7, 2, 6, 3, 5, 4)


def dot(a, b, dims):
    return lax.dot_general(a, b, dims, preferred_element_type=F32)


def iota(shape, dim):
    return lax.broadcasted_iota(jnp.int32, shape, dim)


def kernel(
    tok_h, wq, wk, wd, wv, wg, bias_h, states, head_gain_h, ow, g1_h, b1_h, up, dn, g2_h, b2_h,
    out, new_states,
    tok, bias, head_gain, g1, b1, g2, b2, wst, wc, owc, upc, dnc, st,
    s_a, r_a, s_g, r_g, x, s_b, r_b, ro, s_c, r_c, att32, att,
    s_e, r_e, s_m, r_m, gain1, bias1, gm, s_y, r_y, s_h, r_h, s_f, r_f, sq,
    small_sem, own_sem, w_send, w_recv,
    az_send, az_recv, ax_send, ax_recv, g_sem, p_sem, b_sem, c_send, c_recv, e_send, e_recv, m_sem, y_sem, h_sem, f_sem,
):
    kv = lax.axis_index("kv")
    t = lax.axis_index("tp")
    z, xx = kv // 4, kv % 4
    half = kv // 16
    mine = half == t
    partner = 1 - t

    def wrap(v, n):
        return jnp.where(v >= n, v - n, v)

    zd = [wrap(z + d, 8) for d in range(8)]
    xd = [wrap(xx + d, 4) for d in range(4)]

    def rcopy(src, dst, sems, kv_to, t_to):
        return pltpu.make_async_remote_copy(
            src_ref=src, dst_ref=dst, send_sem=sems.at[0], recv_sem=sems.at[1],
            device_id={"kv": kv_to, "tp": t_to}, device_id_type=MESH,
        )

    def drain(ref, sem):
        pltpu.make_async_copy(ref, ref, sem).wait()

    barrier = pltpu.get_barrier_semaphore()

    def hello(kv_to, t_to):
        pl.semaphore_signal(barrier, inc=1, device_id={"kv": kv_to, "tp": t_to}, device_id_type=MESH)

    for d in (4, 3, 5, 2, 6, 1, 7):
        hello(zd[d] * 4 + xx, t)
        hello(zd[d] * 4 + xx, partner)
    for d in (2, 1, 3):
        hello(z * 4 + xd[d], t)
    hello(kv, partner)

    small = [
        pltpu.make_async_copy(a, b, small_sem.at[i])
        for i, (a, b) in enumerate(
            [(tok_h, tok), (bias_h, bias), (head_gain_h, head_gain), (g1_h, g1), (b1_h, b1), (g2_h, g2), (b2_h, b2)]
        )
    ]
    for c in small:
        c.start()

    own = [
        pltpu.make_async_copy(wq, wst.at[0], own_sem.at[0]),
        pltpu.make_async_copy(wk, wst.at[1], own_sem.at[1]),
        pltpu.make_async_copy(wd, wst.at[2], own_sem.at[2]),
        pltpu.make_async_copy(wv, wc.at[t, pl.ds(96, 64)], own_sem.at[3]),
        pltpu.make_async_copy(wg, wc.at[t, pl.ds(160, 64)], own_sem.at[4]),
        pltpu.make_async_copy(states, st, own_sem.at[5]),
        pltpu.make_async_copy(ow, owc.at[t], own_sem.at[6]),
        pltpu.make_async_copy(up, upc.at[t], own_sem.at[7]),
        pltpu.make_async_copy(dn, dnc.at[t], own_sem.at[8]),
    ]
    for c in own:
        c.start()

    for c in small:
        c.wait()
    tk = tok[...].astype(F32)
    for hh in range(2):
        s_a[hh] = jnp.concatenate(
            [tk[32 * hh : 32 * hh + 16], tk[32 * hh + 16 : 32 * hh + 32]], axis=1
        ).astype(BF16)
    s_g[0:1] = jnp.concatenate([g1[...], b1[...]], axis=1)
    s_g[1:2] = jnp.concatenate([g2[...], b2[...]], axis=1)
    me = kv * 2 + t
    r_a[me] = s_a[t]
    r_g[t, kv] = s_g[...]

    lane = iota((16, 128), 1) < 64
    col = iota((224, 256), 1)
    row = iota((224, 256), 0)
    low = col < 128
    j2 = col - 128
    src_low = ((col % 32) // 8) * 32 + (col % 8) * 4 + col // 32
    src_high = 96 + ((j2 % 16) // 8) * 64 + (j2 % 8) * 8 + j2 // 16
    src_low = jnp.where(col % 32 < 24, src_low, -1)
    perm = jnp.where(row == jnp.where(low, src_low, src_high), 1.0, 0.0).astype(BF16)
    e1 = jnp.where(iota((128, 128), 1) == (iota((128, 128), 0) % 4) * 32 + iota((128, 128), 0) // 4, 1.0, 0.0).astype(BF16)
    e2 = jnp.where(iota((256, 256), 0) == (iota((256, 256), 1) % 8) * 32 + iota((256, 256), 1) // 8, 1.0, 0.0).astype(BF16)
    zero = lambda n: jnp.zeros((n, 128), F32)
    bias_full = jnp.concatenate(
        [zero(16), bias[...], zero(24), bias[...], zero(8 + 64)], axis=0
    ).T[:, :64]

    for c in own[:5]:
        c.wait()
    for ty in range(3):
        for h in range(0, 8, 4):
            wc[t, ty * 32 + h * 4 : ty * 32 + h * 4 + 16, :] = jnp.concatenate(
                [wst[ty, h + i].astype(F32) for i in range(4)], axis=0
            ).astype(BF16)

    def wcopy(ref, i):
        return pltpu.make_async_remote_copy(
            src_ref=ref.at[t], dst_ref=ref.at[t], send_sem=w_send.at[i], recv_sem=w_recv.at[i],
            device_id={"kv": kv, "tp": partner}, device_id_type=MESH,
        )

    wcopies = [wcopy(wc, 0), wcopy(owc, 1), wcopy(upc, 2), wcopy(dnc, 3)]
    pl.semaphore_wait(barrier, 18)

    def to_line(src, kv_to, t_to):
        pltpu.make_async_remote_copy(
            src_ref=src, dst_ref=r_a.at[me], send_sem=az_send, recv_sem=az_recv.at[z * 2 + t],
            device_id={"kv": kv_to, "tp": t_to}, device_id_type=MESH,
        ).start()

    to_line(s_a.at[partner], kv, partner)
    for d in (4, 3, 5, 2, 6, 1, 7):
        for tt in range(2):
            to_line(s_a.at[tt], zd[d] * 4 + xx, tt)
    wcopies[0].start()
    for d in (0, 1, 7, 2, 6, 3, 5, 4):
        if d == 0:
            drain(r_a.at[0], az_recv.at[z * 2 + partner])
        else:
            drain(r_a.at[0], az_recv.at[zd[d] * 2])
            drain(r_a.at[0], az_recv.at[zd[d] * 2 + 1])
        block = r_a.at[pl.ds((zd[d] * 4 + xx) * 2, 2)]
        for e in (2, 1, 3):
            pltpu.make_async_remote_copy(
                src_ref=block, dst_ref=block, send_sem=ax_send, recv_sem=ax_recv.at[zd[d]],
                device_id={"kv": z * 4 + xd[e], "tp": t}, device_id_type=MESH,
            ).start()

    wcopies[0].wait()
    projected = [jnp.zeros((32, 224), F32) for _ in range(2)]
    for d in (0, 1, 7, 2, 6, 3, 5, 4):
        drain(r_a.at[pl.ds(0, 6)], ax_recv.at[zd[d]])
        tiles = []
        for j in range(4):
            a0 = r_a[zd[d] * 8 + 2 * j].astype(F32)
            a1 = r_a[zd[d] * 8 + 2 * j + 1].astype(F32)
            low = jnp.where(lane, a0, pltpu.roll(a1, 64, 1))
            high = jnp.where(lane, pltpu.roll(a0, 64, 1), a1)
            tiles.append(jnp.concatenate([low, high], axis=0).astype(BF16))
        tile = jnp.concatenate(tiles, axis=1)
        cl = pl.ds(pl.multiple_of(zd[d] * 512, 512), 512)
        x[:, cl] = tile
        for tt in range(2):
            projected[tt] = projected[tt] + dot(tile, wc[tt, :, cl], NT)
    for tt in range(2):
        p = projected[tt].astype(BF16)
        p = dot(p, perm, NN)
        for i in range(16):
            s_b[i, tt] = p[2 * i : 2 * i + 2, :].astype(BF16)

    for i in range(4):
        zl = wrap(z - 4 * half + i, 4)
        for j in (2, 1, 3, 0):
            k16 = zl * 4 + xd[j]
            kp = 16 * t + k16
            for tt in range(2):
                if i == 0 and j == 0:

                    @pl.when(jnp.logical_not(jnp.logical_and(mine, t == tt)))
                    def _():
                        rcopy(s_b.at[k16, tt], r_b.at[kv], b_sem, kp, tt).start()

                else:
                    rcopy(s_b.at[k16, tt], r_b.at[kv], b_sem, kp, tt).start()

    for i in range(1, 4):
        own[5 + i].wait()
        wcopies[i].start()
    for d, e in FAR:
        rcopy(s_g, r_g.at[t, kv], g_sem, zd[d] * 4 + xd[e], t).start()
    own[5].wait()

    @pl.when(mine)
    def _():
        r_b[kv] = s_b[lax.rem(kv, 16), t]
        drain(r_b.at[pl.ds(0, 31)], b_sem.at[1])

    @pl.when(jnp.logical_not(mine))
    def _():
        drain(r_b, b_sem.at[1])

    qkd, vg = [], []
    arrived = r_b[...].astype(F32)
    for s in range(2):
        rs = arrived[:, s, :]
        qkd.append(jnp.concatenate([rs[:, c * 32 : (c + 1) * 32] for c in range(4)], axis=0))
        vg.append(jnp.concatenate([rs[:, 128 + c * 16 : 144 + c * 16] for c in range(8)], axis=0))
    cols = dot(e1, jnp.concatenate(qkd, axis=1).astype(BF16), NN)
    rows = [dot(v.astype(BF16), e2, TN) for v in vg]
    decay = cols + bias_full
    log_sig = jnp.minimum(decay, 0.0) - jnp.log1p(jnp.exp(-jnp.abs(decay)))
    retain = jnp.exp(log_sig / TAU)
    q = cols * KEY_DIM ** (-0.5)
    for s in range(2):
        for h in range(8):
            o = s * 32 + h
            new = retain[:, o + 16 : o + 17] * st[s, h] + cols[:, o + 8 : o + 9] * rows[s][h : h + 1, :]
            new_states[s, h] = new
            ro[s * 8 + h : s * 8 + h + 1, :] = jnp.sum(q[:, o : o + 1] * new, axis=0, keepdims=True)
    readout = ro[...]
    gate = jnp.concatenate([rows[0][8:16], rows[1][8:16]], axis=0)
    hg = jnp.concatenate([head_gain[...], head_gain[...]], axis=0)
    readout = readout * lax.rsqrt(jnp.mean(readout * readout, axis=-1, keepdims=True) + RMS_EPS) * hg
    s_c[...] = (readout * (gate / (1.0 + jnp.exp(-gate)))).astype(BF16)

    slot_c = t * 16 + lax.rem(kv, 16)

    drain(r_g.at[t, pl.ds(0, 31)], g_sem.at[1])
    gains = rcopy(r_g.at[t], r_g.at[t], p_sem, kv, partner)
    gains.start()

    def send_c(src, slot, kv_to, t_to):
        pltpu.make_async_remote_copy(
            src_ref=src, dst_ref=r_c.at[slot], send_sem=c_send, recv_sem=c_recv.at[slot],
            device_id={"kv": kv_to, "tp": t_to}, device_id_type=MESH,
        ).start()

    for d, e in FAR:
        if e == 0 or d not in NEAR:
            send_c(s_c, slot_c, zd[d] * 4 + xd[e], half)

    @pl.when(jnp.logical_not(mine))
    def _():
        send_c(s_c, slot_c, kv, half)

    @pl.when(mine)
    def _():
        r_c[slot_c] = s_c[...]

    for d in NEAR:

        @pl.when(zd[d] // 4 == t)
        def _():
            for tt in range(2):
                slot = tt * 16 + (zd[d] - 4 * t) * 4 + xx
                drain(s_c, c_recv.at[slot])
                for e in (2, 1, 3):
                    send_c(r_c.at[slot], slot, z * 4 + xd[e], t)

    gains.wait()
    ga = r_g[0, :, 0, :]
    gb = r_g[1, :, 0, :]
    lane32 = iota((32, 128), 1) < 64
    gain1[...] = jnp.where(lane32, ga, pltpu.roll(gb, 64, 1))
    bias1[...] = jnp.where(lane32, pltpu.roll(ga, 64, 1), gb)
    wcopies[2].wait()
    shift = [jnp.zeros((1, 256), F32) for _ in range(2)]
    for c in range(CHIPS):
        parts = []
        for v in (gain1[c : c + 1, :], bias1[c : c + 1, :]):
            high = v.astype(BF16).astype(F32)
            parts += [high, v - high]
        parts = jnp.concatenate(parts + [jnp.zeros((4, 128), F32)], axis=0).astype(BF16)
        for tt in range(2):
            r = dot(parts, upc[tt, c * 128 : (c + 1) * 128, :], NN)
            gm[tt, c : c + 1, :] = r[0:1] + r[1:2]
            shift[tt] = shift[tt] + (r[2:3] + r[3:4])

    for d in range(8):
        for e in range(4):
            if e == 0 and d in NEAR:
                continue

            @pl.when(zd[d] // 4 == t)
            def _():
                for tt in range(2):
                    slot = tt * 16 + (zd[d] - 4 * t) * 4 + xd[e]
                    if d or e:
                        drain(s_c, c_recv.at[slot])
                    else:

                        @pl.when(t != tt)
                        def _():
                            drain(s_c, c_recv.at[slot])

    for tt in range(2):
        arrived = r_c[tt * 16 : (tt + 1) * 16].astype(F32).reshape(256, 256)
        for n in range(2):
            att32[n] = arrived[:, n * 128 : (n + 1) * 128]
            for h in range(8):
                at = tt * 2048 + h * 256 + n * 128
                att[:, at : at + 128] = att32[n, pl.ds(h, 32, stride=8), :].astype(BF16)
    wcopies[1].wait()
    mixed = jnp.concatenate([dot(att[...], owc[tt], NT) for tt in range(2)], axis=1)
    at_chip = pl.multiple_of(kv * 128, 128)
    res1 = ALPHA * x[:, pl.ds(at_chip, 128)].astype(F32) + mixed

    m_own = jnp.mean(res1, axis=-1, keepdims=True)
    sq[0:32, :] = jnp.broadcast_to(m_own, (32, 128))
    sq[32:128, :] = jnp.zeros((96, 128), F32)
    s_m[...] = sq[...].T[0:1, :]
    s_e[...] = (res1 - m_own).astype(BF16)

    def send_e(src, slot, kv_to):
        pltpu.make_async_remote_copy(
            src_ref=src, dst_ref=r_e.at[slot], send_sem=e_send, recv_sem=e_recv.at[slot],
            device_id={"kv": kv_to, "tp": t}, device_id_type=MESH,
        ).start()

    for d, e in FAR:
        if e == 0 or d not in NEAR:
            send_e(s_e, kv, zd[d] * 4 + xd[e])
    for d, e in FAR:
        rcopy(s_m, r_m.at[kv], m_sem, zd[d] * 4 + xd[e], t).start()
    for d in NEAR:
        slot = zd[d] * 4 + xx
        drain(s_e, e_recv.at[slot])
        for e in (2, 1, 3):
            send_e(r_e.at[slot], slot, z * 4 + xd[e])
    r_e[kv] = s_e[...]
    r_m[kv] = s_m[...]
    raw = [jnp.zeros((32, 256), F32) for _ in range(2)]
    acc = jnp.zeros((32, 128), F32)
    for d in (0, 1, 7, 2, 6, 3, 5, 4):
        tiles = []
        for e in range(1, 4):
            drain(s_e, e_recv.at[zd[d] * 4 + xd[e]])
        for j in range(4):
            v = r_e[zd[d] * 4 + j].astype(F32)
            acc = acc + v
            tiles.append((v * gain1[pl.ds(zd[d] * 4 + j, 1), :]).astype(BF16))
        tile = jnp.concatenate(tiles, axis=1)
        for tt in range(2):
            raw[tt] = raw[tt] + dot(tile, upc[tt, pl.ds(pl.multiple_of(zd[d] * 512, 512), 512), :], NN)
    drain(r_m.at[pl.ds(0, 31)], m_sem.at[1])
    sq[0:32, :] = r_m[:, 0, :]
    means = sq[...].T[0:32, 0:32]
    mean = (jnp.sum(acc, axis=-1, keepdims=True) + 128.0 * jnp.sum(means, axis=-1, keepdims=True)) / D
    means = means - mean
    acc = jnp.zeros((32, 128), F32)
    for c in range(CHIPS):
        v = r_e[c].astype(F32) + means[:, c : c + 1]
        acc = acc + v * v
    inv = lax.rsqrt(jnp.sum(acc, axis=-1, keepdims=True) / D + LN_EPS)
    own_gain = gain1[pl.ds(kv, 1), :]
    own_bias = bias1[pl.ds(kv, 1), :]
    normed = ((s_e[...].astype(F32) + (m_own - mean)) * inv * own_gain + own_bias).astype(BF16)

    wcopies[3].wait()
    hidden = []
    for tt in range(2):
        level = lax.dot_general(means, gm[tt], NN, precision=lax.Precision.HIGHEST, preferred_element_type=F32)
        lifted = jnp.maximum((raw[tt] + level) * inv + shift[tt], 0.0)
        hidden.append((lifted * lifted).astype(BF16))
    for d in (4, 3, 5, 2, 6, 1, 7, 0):
        cl = pl.ds(pl.multiple_of(zd[d] * 512, 512), 512)
        y = (dot(hidden[0], dnc[0, :, cl], NN) + dot(hidden[1], dnc[1, :, cl], NN)).astype(BF16)
        for j in range(4):
            s_y[zd[d] * 4 + j] = y[:, j * 128 : (j + 1) * 128]
        for e in (2, 1, 3, 0):
            if d or e:
                kp = zd[d] * 4 + xd[e]
                rcopy(s_y.at[kp], r_y.at[kv], y_sem, kp, t).start()

    r_y[kv] = s_y[kv]
    drain(r_y.at[pl.ds(0, 31)], y_sem.at[1])
    res2 = ALPHA * normed.astype(F32)
    for c in range(CHIPS):
        res2 = res2 + r_y[c].astype(F32)

    m_own = jnp.mean(res2, axis=-1, keepdims=True)
    dev = res2 - m_own
    v_own = jnp.sum(dev * dev, axis=-1, keepdims=True)
    sq[0:32, :] = jnp.where(iota((32, 128), 1) == 0, m_own, v_own)
    flat = sq[...].T
    s_h[...] = jnp.concatenate([flat[0:1, 0:32], flat[1:2, 0:32], flat[0:1, 0:64]], axis=1)
    s_f[...] = res2
    last = rcopy(s_f, r_f, f_sem, kv, partner)
    for d, e in FAR:
        for tt in range(2):
            rcopy(s_h, r_h.at[t * CHIPS + kv], h_sem, zd[d] * 4 + xd[e], tt).start()
    rcopy(s_h, r_h.at[t * CHIPS + kv], h_sem, kv, partner).start()
    last.start()
    r_h[t * CHIPS + kv] = s_h[...]
    own0 = r_g[0, kv][1:2, :]
    own1 = r_g[1, kv][1:2, :]
    lane1 = iota((1, 128), 1) < 64
    gain2 = jnp.where(lane1, own0, pltpu.roll(own1, 64, 1))
    bias2 = jnp.where(lane1, pltpu.roll(own0, 64, 1), own1)
    last.wait()
    drain(r_h.at[pl.ds(0, 63)], h_sem.at[1])
    for tt in range(2):
        ms = r_h[tt * CHIPS : (tt + 1) * CHIPS, 0, :]
        mean = jnp.mean(ms, axis=0, keepdims=True)
        dm = ms - mean
        first = jnp.sum(ms, axis=0, keepdims=True)
        spread = (first + pltpu.roll(128.0 * jnp.sum(dm * dm, axis=0, keepdims=True), 32, 1)) / D
        sq[2 * tt : 2 * tt + 1, :] = mean
        sq[2 * tt + 1 : 2 * tt + 2, :] = lax.rsqrt(spread + LN_EPS)
    back = sq[...].T
    for tt in range(2):
        rows2 = jnp.where(t == tt, res2, r_f[...])
        o = (rows2 - back[0:32, 2 * tt : 2 * tt + 1]) * back[32:64, 2 * tt + 1 : 2 * tt + 2] * gain2 + bias2
        out[32 * tt : 32 * tt + 32, :] = jnp.where(t == 0, o, pltpu.roll(o, 64, 1))[:, :64].astype(BF16)

    drain(r_a.at[pl.ds(0, 15)], az_send)
    drain(r_a.at[pl.ds(0, 48)], ax_send)
    drain(r_g.at[t, pl.ds(0, 31)], g_sem.at[0])
    sent = 3 + sum(1 if d in NEAR else 4 for d in range(1, 8))
    drain(r_c.at[pl.ds(0, sent)], c_send)

    @pl.when(mine)
    def _():
        drain(r_b.at[pl.ds(0, 31)], b_sem.at[0])

    @pl.when(jnp.logical_not(mine))
    def _():
        drain(r_b, b_sem.at[0])
        drain(s_c, c_send)

    for d in NEAR:

        @pl.when(zd[d] // 4 == t)
        def _():
            drain(r_c.at[pl.ds(0, 6)], c_send)

    drain(r_e.at[pl.ds(0, 31)], e_send)
    drain(r_m.at[pl.ds(0, 31)], m_sem.at[0])
    drain(r_y.at[pl.ds(0, 31)], y_sem.at[0])
    drain(r_h.at[pl.ds(0, 63)], h_sem.at[0])


def body(
    tokens, query_weight, key_weight, value_weight, gate_weight, decay_weight, decay_bias, states,
    head_gain, out_weight, norm1_gain, norm1_bias, up_weight, down_weight, norm2_gain, norm2_bias,
):
    flip = lambda w: w.transpose(1, 2, 0)
    flat = lambda w: flip(w).reshape(-1, D)
    line = lambda v: v.reshape(1, -1)
    vmem = pl.BlockSpec(memory_space=pltpu.VMEM)
    hbm = pl.BlockSpec(memory_space=pl.ANY)
    V = pltpu.VMEM
    dma = pltpu.SemaphoreType.DMA
    scratch = [
        V((64, 64), BF16), V((8, 128), F32), V((8, 256), F32),
        V((1, 64), F32), V((1, 64), F32), V((1, 64), F32), V((1, 64), F32),
        V((3, 8, 4, D), BF16),
        V((2, 224, D), BF16),
        V((2, 64, D), BF16),
        V((2, D, 256), BF16),
        V((2, 256, D), BF16),
        V((2, 8, 128, 256), F32),
        V((2, 16, 128), BF16), V((64, 16, 128), BF16),
        V((2, 128), F32), V((2, 32, 2, 128), F32),
        V((32, D), BF16),
        V((16, 2, 2, 256), BF16), V((32, 2, 256), BF16),
        V((16, 256), F32),
        V((16, 256), BF16), V((32, 16, 256), BF16),
        V((2, 256, 128), F32), V((32, D), BF16),
        V((32, 128), BF16), V((32, 32, 128), BF16),
        V((1, 128), F32), V((32, 1, 128), F32),
        V((32, 128), F32), V((32, 128), F32), V((2, 32, 256), F32),
        V((32, 32, 128), BF16), V((32, 32, 128), BF16),
        V((1, 128), F32), V((64, 1, 128), F32),
        V((32, 128), F32), V((32, 128), F32),
        V((128, 128), F32),
        dma((7,)), dma((9,)), dma((4,)), dma((4,)), dma, dma((16,)), dma, dma((8,)),
        dma((2,)), dma((2,)), dma((2,)), dma, dma((32,)), dma, dma((32,)),
    ] + [dma((2,))] * 4
    return pl.pallas_call(
        kernel,
        out_shape=(
            pltpu.VMEM((64, 64), BF16),
            pltpu.VMEM((2, 8, 128, 256), F32),
        ),
        in_specs=[hbm] * 16,
        out_specs=(vmem, vmem),
        scratch_shapes=scratch,
        compiler_params=pltpu.CompilerParams(
            collective_id=0, has_side_effects=True, vmem_limit_bytes=60 * 1024 * 1024
        ),
        name="layer_step",
    )(
        tokens, flip(query_weight), flip(key_weight), flip(decay_weight), flat(value_weight), flat(gate_weight),
        decay_bias, states, head_gain, out_weight.T, line(norm1_gain), line(norm1_bias), up_weight, down_weight,
        line(norm2_gain), line(norm2_bias),
    )


def solution(mesh):
    placed = (
        P("dp", ("kv", "tp")),
        P(None, "tp", "kv"),
        P(None, "tp", "kv"),
        P(None, "tp", "kv"),
        P(None, "tp", "kv"),
        P(None, "tp", "kv"),
        P("tp", None),
        P(("dp", "kv"), "tp", None, None),
        P("tp", None),
        P(None, ("kv", "tp")),
        P(("kv", "tp")),
        P(("kv", "tp")),
        P(None, ("kv", "tp")),
        P(("kv", "tp"), None),
        P(("kv", "tp")),
        P(("kv", "tp")),
    )
    return jax.shard_map(
        body,
        mesh=mesh,
        in_specs=placed,
        out_specs=(P("dp", ("kv", "tp")), P(("dp", "kv"), "tp", None, None)),
        check_vma=False,
    )
```

```python
import functools

import jax
import jax.numpy as jnp
from jax import lax
from jax.experimental import pallas as pl
from jax.experimental.pallas import tpu as pltpu
from jax.sharding import PartitionSpec as P

D = 4096
KEY_DIM = 128
ALPHA = 2.0**0.5
TAU = 16.0
LN_EPS = 1e-05
RMS_EPS = 1e-06
MESH = pl.DeviceIdType.MESH
F32 = jnp.float32
BF16 = jnp.bfloat16
NT = (((1,), (1,)), ((), ()))
NN = (((1,), (0,)), ((), ()))
TN = (((0,), (0,)), ((), ()))
CHIPS = 32
FAR = sorted(
    ((d, e) for d in range(8) for e in range(4) if d or e),
    key=lambda o: (-min(o[0], 8 - o[0]) - min(o[1], 4 - o[1]), o),
)
NEAR = (1, 7, 2, 6, 3, 5, 4)


def dot(a, b, dims):
    return lax.dot_general(a, b, dims, preferred_element_type=F32)


def iota(shape, dim):
    return lax.broadcasted_iota(jnp.int32, shape, dim)


def kernel(
    tok_h, wq, wk, wd, wv, wg, bias_h, states, head_gain_h, ow, g1_h, b1_h, up, dn, g2_h, b2_h,
    out, new_states,
    tok, bias, head_gain, g1, b1, g2, b2, wst, wc, owc, upc, dnc, st,
    s_a, r_a, s_g, r_g, x, s_b, r_b, ro, s_c, r_c, att32, att,
    s_e, r_e, s_m, r_m, gain1, bias1, gm, s_y, r_y, s_h, r_h, s_f, r_f, sq,
    small_sem, own_sem, w_send, w_recv,
    az_send, az_recv, ax_send, ax_recv, g_sem, p_sem, b_sem, c_send, c_recv, e_send, e_recv, m_sem, y_sem, h_sem, f_sem,
):
    kv = lax.axis_index("kv")
    t = lax.axis_index("tp")
    z, xx = kv // 4, kv % 4
    half = kv // 16
    mine = half == t
    partner = 1 - t

    def wrap(v, n):
        return jnp.where(v >= n, v - n, v)

    zd = [wrap(z + d, 8) for d in range(8)]
    xd = [wrap(xx + d, 4) for d in range(4)]

    def rcopy(src, dst, sems, kv_to, t_to):
        return pltpu.make_async_remote_copy(
            src_ref=src, dst_ref=dst, send_sem=sems.at[0], recv_sem=sems.at[1],
            device_id={"kv": kv_to, "tp": t_to}, device_id_type=MESH,
        )

    def drain(ref, sem):
        pltpu.make_async_copy(ref, ref, sem).wait()

    barrier = pltpu.get_barrier_semaphore()

    def hello(kv_to, t_to):
        pl.semaphore_signal(barrier, inc=1, device_id={"kv": kv_to, "tp": t_to}, device_id_type=MESH)

    for d in (4, 3, 5, 2, 6, 1, 7):
        hello(zd[d] * 4 + xx, t)
        hello(zd[d] * 4 + xx, partner)
    for d in (2, 1, 3):
        hello(z * 4 + xd[d], t)
    hello(kv, partner)

    small = [
        pltpu.make_async_copy(a, b, small_sem.at[i])
        for i, (a, b) in enumerate(
            [(tok_h, tok), (bias_h, bias), (head_gain_h, head_gain), (g1_h, g1), (b1_h, b1), (g2_h, g2), (b2_h, b2)]
        )
    ]
    for c in small:
        c.start()

    own = [
        pltpu.make_async_copy(wq, wst.at[0], own_sem.at[0]),
        pltpu.make_async_copy(wk, wst.at[1], own_sem.at[1]),
        pltpu.make_async_copy(wd, wst.at[2], own_sem.at[2]),
        pltpu.make_async_copy(wv, wc.at[t, pl.ds(96, 64)], own_sem.at[3]),
        pltpu.make_async_copy(wg, wc.at[t, pl.ds(160, 64)], own_sem.at[4]),
        pltpu.make_async_copy(states, st, own_sem.at[5]),
        pltpu.make_async_copy(ow, owc.at[t], own_sem.at[6]),
        pltpu.make_async_copy(up, upc.at[t], own_sem.at[7]),
        pltpu.make_async_copy(dn, dnc.at[t], own_sem.at[8]),
    ]
    for c in own:
        c.start()

    for c in small:
        c.wait()
    tk = tok[...].astype(F32)
    for hh in range(2):
        s_a[hh] = jnp.concatenate(
            [tk[32 * hh : 32 * hh + 16], tk[32 * hh + 16 : 32 * hh + 32]], axis=1
        ).astype(BF16)
    s_g[0:1] = jnp.concatenate([g1[...], b1[...]], axis=1)
    s_g[1:2] = jnp.concatenate([g2[...], b2[...]], axis=1)
    me = kv * 2 + t
    r_a[me] = s_a[t]
    r_g[t, kv] = s_g[...]

    lane = iota((16, 128), 1) < 64
    col = iota((224, 256), 1)
    row = iota((224, 256), 0)
    low = col < 128
    j2 = col - 128
    src_low = ((col % 32) // 8) * 32 + (col % 8) * 4 + col // 32
    src_high = 96 + ((j2 % 16) // 8) * 64 + (j2 % 8) * 8 + j2 // 16
    src_low = jnp.where(col % 32 < 24, src_low, -1)
    perm = jnp.where(row == jnp.where(low, src_low, src_high), 1.0, 0.0).astype(BF16)
    e1 = jnp.where(iota((128, 128), 1) == (iota((128, 128), 0) % 4) * 32 + iota((128, 128), 0) // 4, 1.0, 0.0).astype(BF16)
    e2 = jnp.where(iota((256, 256), 0) == (iota((256, 256), 1) % 8) * 32 + iota((256, 256), 1) // 8, 1.0, 0.0).astype(BF16)
    zero = lambda n: jnp.zeros((n, 128), F32)
    bias_full = jnp.concatenate(
        [zero(16), bias[...], zero(24), bias[...], zero(8 + 64)], axis=0
    ).T[:, :64]

    for c in own[:5]:
        c.wait()
    for ty in range(3):
        for h in range(0, 8, 4):
            wc[t, ty * 32 + h * 4 : ty * 32 + h * 4 + 16, :] = jnp.concatenate(
                [wst[ty, h + i].astype(F32) for i in range(4)], axis=0
            ).astype(BF16)

    def wcopy(ref, i):
        return pltpu.make_async_remote_copy(
            src_ref=ref.at[t], dst_ref=ref.at[t], send_sem=w_send.at[i], recv_sem=w_recv.at[i],
            device_id={"kv": kv, "tp": partner}, device_id_type=MESH,
        )

    wcopies = [wcopy(wc, 0), wcopy(owc, 1), wcopy(upc, 2), wcopy(dnc, 3)]
    pl.semaphore_wait(barrier, 18)

    def to_line(src, kv_to, t_to):
        pltpu.make_async_remote_copy(
            src_ref=src, dst_ref=r_a.at[me], send_sem=az_send, recv_sem=az_recv.at[z * 2 + t],
            device_id={"kv": kv_to, "tp": t_to}, device_id_type=MESH,
        ).start()

    to_line(s_a.at[partner], kv, partner)
    for d in (4, 3, 5, 2, 6, 1, 7):
        for tt in range(2):
            to_line(s_a.at[tt], zd[d] * 4 + xx, tt)
    wcopies[0].start()
    for d in (0, 1, 7, 2, 6, 3, 5, 4):
        if d == 0:
            drain(r_a.at[0], az_recv.at[z * 2 + partner])
        else:
            drain(r_a.at[0], az_recv.at[zd[d] * 2])
            drain(r_a.at[0], az_recv.at[zd[d] * 2 + 1])
        block = r_a.at[pl.ds((zd[d] * 4 + xx) * 2, 2)]
        for e in (2, 1, 3):
            pltpu.make_async_remote_copy(
                src_ref=block, dst_ref=block, send_sem=ax_send, recv_sem=ax_recv.at[zd[d]],
                device_id={"kv": z * 4 + xd[e], "tp": t}, device_id_type=MESH,
            ).start()

    wcopies[0].wait()
    projected = [jnp.zeros((32, 224), F32) for _ in range(2)]
    for d in (0, 1, 7, 2, 6, 3, 5, 4):
        drain(r_a.at[pl.ds(0, 6)], ax_recv.at[zd[d]])
        tiles = []
        for j in range(4):
            a0 = r_a[zd[d] * 8 + 2 * j].astype(F32)
            a1 = r_a[zd[d] * 8 + 2 * j + 1].astype(F32)
            low = jnp.where(lane, a0, pltpu.roll(a1, 64, 1))
            high = jnp.where(lane, pltpu.roll(a0, 64, 1), a1)
            tiles.append(jnp.concatenate([low, high], axis=0).astype(BF16))
        tile = jnp.concatenate(tiles, axis=1)
        cl = pl.ds(pl.multiple_of(zd[d] * 512, 512), 512)
        x[:, cl] = tile
        for tt in range(2):
            projected[tt] = projected[tt] + dot(tile, wc[tt, :, cl], NT)
    for tt in range(2):
        p = projected[tt].astype(BF16)
        p = dot(p, perm, NN)
        for i in range(16):
            s_b[i, tt] = p[2 * i : 2 * i + 2, :].astype(BF16)

    for i in (2, 1, 3, 0):
        zl = wrap(z - 4 * half + i, 4)
        for j in (2, 1, 3, 0):
            k16 = zl * 4 + xd[j]
            kp = 16 * t + k16
            for tt in range(2):
                if i == 0 and j == 0:

                    @pl.when(jnp.logical_not(jnp.logical_and(mine, t == tt)))
                    def _():
                        rcopy(s_b.at[k16, tt], r_b.at[kv], b_sem, kp, tt).start()

                else:
                    rcopy(s_b.at[k16, tt], r_b.at[kv], b_sem, kp, tt).start()

    for i in range(1, 4):
        own[5 + i].wait()
        wcopies[i].start()
    for d, e in FAR:
        rcopy(s_g, r_g.at[t, kv], g_sem, zd[d] * 4 + xd[e], t).start()
    own[5].wait()

    @pl.when(mine)
    def _():
        r_b[kv] = s_b[lax.rem(kv, 16), t]
        drain(r_b.at[pl.ds(0, 31)], b_sem.at[1])

    @pl.when(jnp.logical_not(mine))
    def _():
        drain(r_b, b_sem.at[1])

    qkd, vg = [], []
    arrived = r_b[...].astype(F32)
    for s in range(2):
        rs = arrived[:, s, :]
        qkd.append(jnp.concatenate([rs[:, c * 32 : (c + 1) * 32] for c in range(4)], axis=0))
        vg.append(jnp.concatenate([rs[:, 128 + c * 16 : 144 + c * 16] for c in range(8)], axis=0))
    cols = dot(e1, jnp.concatenate(qkd, axis=1).astype(BF16), NN)
    rows = [dot(v.astype(BF16), e2, TN) for v in vg]
    decay = cols + bias_full
    log_sig = jnp.minimum(decay, 0.0) - jnp.log1p(jnp.exp(-jnp.abs(decay)))
    retain = jnp.exp(log_sig / TAU)
    q = cols * KEY_DIM ** (-0.5)
    for s in range(2):
        for h in range(8):
            o = s * 32 + h
            new = retain[:, o + 16 : o + 17] * st[s, h] + cols[:, o + 8 : o + 9] * rows[s][h : h + 1, :]
            new_states[s, h] = new
            ro[s * 8 + h : s * 8 + h + 1, :] = jnp.sum(q[:, o : o + 1] * new, axis=0, keepdims=True)
    readout = ro[...]
    gate = jnp.concatenate([rows[0][8:16], rows[1][8:16]], axis=0)
    hg = jnp.concatenate([head_gain[...], head_gain[...]], axis=0)
    readout = readout * lax.rsqrt(jnp.mean(readout * readout, axis=-1, keepdims=True) + RMS_EPS) * hg
    s_c[...] = (readout * (gate / (1.0 + jnp.exp(-gate)))).astype(BF16)

    slot_c = t * 16 + lax.rem(kv, 16)

    drain(r_g.at[t, pl.ds(0, 31)], g_sem.at[1])
    gains = rcopy(r_g.at[t], r_g.at[t], p_sem, kv, partner)
    gains.start()

    def send_c(src, slot, kv_to, t_to):
        pltpu.make_async_remote_copy(
            src_ref=src, dst_ref=r_c.at[slot], send_sem=c_send, recv_sem=c_recv.at[slot],
            device_id={"kv": kv_to, "tp": t_to}, device_id_type=MESH,
        ).start()

    for d, e in FAR:
        if e == 0 or d not in NEAR:
            send_c(s_c, slot_c, zd[d] * 4 + xd[e], half)

    @pl.when(jnp.logical_not(mine))
    def _():
        send_c(s_c, slot_c, kv, half)

    @pl.when(mine)
    def _():
        r_c[slot_c] = s_c[...]

    for d in NEAR:

        @pl.when(zd[d] // 4 == t)
        def _():
            for tt in range(2):
                slot = tt * 16 + (zd[d] - 4 * t) * 4 + xx
                drain(s_c, c_recv.at[slot])
                for e in (2, 1, 3):
                    send_c(r_c.at[slot], slot, z * 4 + xd[e], t)

    gains.wait()
    ga = r_g[0, :, 0, :]
    gb = r_g[1, :, 0, :]
    lane32 = iota((32, 128), 1) < 64
    gain1[...] = jnp.where(lane32, ga, pltpu.roll(gb, 64, 1))
    bias1[...] = jnp.where(lane32, pltpu.roll(ga, 64, 1), gb)
    wcopies[2].wait()
    shift = [jnp.zeros((1, 256), F32) for _ in range(2)]
    for c in range(CHIPS):
        parts = []
        for v in (gain1[c : c + 1, :], bias1[c : c + 1, :]):
            high = v.astype(BF16).astype(F32)
            parts += [high, v - high]
        parts = jnp.concatenate(parts + [jnp.zeros((4, 128), F32)], axis=0).astype(BF16)
        for tt in range(2):
            r = dot(parts, upc[tt, c * 128 : (c + 1) * 128, :], NN)
            gm[tt, c : c + 1, :] = r[0:1] + r[1:2]
            shift[tt] = shift[tt] + (r[2:3] + r[3:4])

    for d in range(8):
        for e in range(4):
            if e == 0 and d in NEAR:
                continue

            @pl.when(zd[d] // 4 == t)
            def _():
                for tt in range(2):
                    slot = tt * 16 + (zd[d] - 4 * t) * 4 + xd[e]
                    if d or e:
                        drain(s_c, c_recv.at[slot])
                    else:

                        @pl.when(t != tt)
                        def _():
                            drain(s_c, c_recv.at[slot])

    for tt in range(2):
        arrived = r_c[tt * 16 : (tt + 1) * 16].astype(F32).reshape(256, 256)
        for n in range(2):
            att32[n] = arrived[:, n * 128 : (n + 1) * 128]
            for h in range(8):
                at = tt * 2048 + h * 256 + n * 128
                att[:, at : at + 128] = att32[n, pl.ds(h, 32, stride=8), :].astype(BF16)
    wcopies[1].wait()
    mixed = jnp.concatenate([dot(att[...], owc[tt], NT) for tt in range(2)], axis=1)
    at_chip = pl.multiple_of(kv * 128, 128)
    res1 = ALPHA * x[:, pl.ds(at_chip, 128)].astype(F32) + mixed

    m_own = jnp.mean(res1, axis=-1, keepdims=True)
    s_e[...] = (res1 - m_own).astype(BF16)

    def send_e(src, slot, kv_to):
        pltpu.make_async_remote_copy(
            src_ref=src, dst_ref=r_e.at[slot], send_sem=e_send, recv_sem=e_recv.at[slot],
            device_id={"kv": kv_to, "tp": t}, device_id_type=MESH,
        ).start()

    for d, e in FAR:
        if e == 0 or d not in NEAR:
            send_e(s_e, kv, zd[d] * 4 + xd[e])
    sq[0:32, :] = jnp.broadcast_to(m_own, (32, 128))
    sq[32:128, :] = jnp.zeros((96, 128), F32)
    s_m[...] = sq[...].T[0:1, :]
    for d, e in FAR:
        rcopy(s_m, r_m.at[kv], m_sem, zd[d] * 4 + xd[e], t).start()
    for d in NEAR:
        slot = zd[d] * 4 + xx
        drain(s_e, e_recv.at[slot])
        for e in (2, 1, 3):
            send_e(r_e.at[slot], slot, z * 4 + xd[e])
    r_e[kv] = s_e[...]
    r_m[kv] = s_m[...]
    raw = [jnp.zeros((32, 256), F32) for _ in range(2)]
    acc = jnp.zeros((32, 128), F32)
    for d in (0, 1, 7, 2, 6, 3, 5, 4):
        tiles = []
        for e in range(1, 4):
            drain(s_e, e_recv.at[zd[d] * 4 + xd[e]])
        for j in range(4):
            v = r_e[zd[d] * 4 + j].astype(F32)
            acc = acc + v
            tiles.append((v * gain1[pl.ds(zd[d] * 4 + j, 1), :]).astype(BF16))
        tile = jnp.concatenate(tiles, axis=1)
        for tt in range(2):
            raw[tt] = raw[tt] + dot(tile, upc[tt, pl.ds(pl.multiple_of(zd[d] * 512, 512), 512), :], NN)
    drain(r_m.at[pl.ds(0, 31)], m_sem.at[1])
    sq[0:32, :] = r_m[:, 0, :]
    means = sq[...].T[0:32, 0:32]
    mean = (jnp.sum(acc, axis=-1, keepdims=True) + 128.0 * jnp.sum(means, axis=-1, keepdims=True)) / D
    means = means - mean
    acc = jnp.zeros((32, 128), F32)
    for c in range(CHIPS):
        v = r_e[c].astype(F32) + means[:, c : c + 1]
        acc = acc + v * v
    inv = lax.rsqrt(jnp.sum(acc, axis=-1, keepdims=True) / D + LN_EPS)
    own_gain = gain1[pl.ds(kv, 1), :]
    own_bias = bias1[pl.ds(kv, 1), :]
    normed = ((s_e[...].astype(F32) + (m_own - mean)) * inv * own_gain + own_bias).astype(BF16)

    wcopies[3].wait()
    hidden = []
    for tt in range(2):
        level = lax.dot_general(means, gm[tt], NN, precision=lax.Precision.HIGHEST, preferred_element_type=F32)
        lifted = jnp.maximum((raw[tt] + level) * inv + shift[tt], 0.0)
        hidden.append((lifted * lifted).astype(BF16))
    for d in (4, 3, 5, 2, 6, 1, 7, 0):
        cl = pl.ds(pl.multiple_of(zd[d] * 512, 512), 512)
        y = (dot(hidden[0], dnc[0, :, cl], NN) + dot(hidden[1], dnc[1, :, cl], NN)).astype(BF16)
        for j in range(4):
            s_y[zd[d] * 4 + j] = y[:, j * 128 : (j + 1) * 128]
        for e in (2, 1, 3, 0):
            if d or e:
                kp = zd[d] * 4 + xd[e]
                rcopy(s_y.at[kp], r_y.at[kv], y_sem, kp, t).start()

    r_y[kv] = s_y[kv]
    drain(r_y.at[pl.ds(0, 31)], y_sem.at[1])
    res2 = ALPHA * normed.astype(F32)
    for c in range(CHIPS):
        res2 = res2 + r_y[c].astype(F32)

    m_own = jnp.mean(res2, axis=-1, keepdims=True)
    dev = res2 - m_own
    v_own = jnp.sum(dev * dev, axis=-1, keepdims=True)
    sq[0:32, :] = jnp.where(iota((32, 128), 1) == 0, m_own, v_own)
    flat = sq[...].T
    s_h[...] = jnp.concatenate([flat[0:1, 0:32], flat[1:2, 0:32], flat[0:1, 0:64]], axis=1)
    s_f[...] = res2
    last = rcopy(s_f, r_f, f_sem, kv, partner)
    for d, e in FAR:
        for tt in range(2):
            rcopy(s_h, r_h.at[t * CHIPS + kv], h_sem, zd[d] * 4 + xd[e], tt).start()
    rcopy(s_h, r_h.at[t * CHIPS + kv], h_sem, kv, partner).start()
    last.start()
    r_h[t * CHIPS + kv] = s_h[...]
    own0 = r_g[0, kv][1:2, :]
    own1 = r_g[1, kv][1:2, :]
    lane1 = iota((1, 128), 1) < 64
    gain2 = jnp.where(lane1, own0, pltpu.roll(own1, 64, 1))
    bias2 = jnp.where(lane1, pltpu.roll(own0, 64, 1), own1)
    last.wait()
    drain(r_h.at[pl.ds(0, 63)], h_sem.at[1])
    for tt in range(2):
        ms = r_h[tt * CHIPS : (tt + 1) * CHIPS, 0, :]
        mean = jnp.mean(ms, axis=0, keepdims=True)
        dm = ms - mean
        first = jnp.sum(ms, axis=0, keepdims=True)
        spread = (first + pltpu.roll(128.0 * jnp.sum(dm * dm, axis=0, keepdims=True), 32, 1)) / D
        sq[2 * tt : 2 * tt + 1, :] = mean
        sq[2 * tt + 1 : 2 * tt + 2, :] = lax.rsqrt(spread + LN_EPS)
    back = sq[...].T
    for tt in range(2):
        rows2 = jnp.where(t == tt, res2, r_f[...])
        o = (rows2 - back[0:32, 2 * tt : 2 * tt + 1]) * back[32:64, 2 * tt + 1 : 2 * tt + 2] * gain2 + bias2
        out[32 * tt : 32 * tt + 32, :] = jnp.where(t == 0, o, pltpu.roll(o, 64, 1))[:, :64].astype(BF16)

    drain(r_a.at[pl.ds(0, 15)], az_send)
    drain(r_a.at[pl.ds(0, 48)], ax_send)
    drain(r_g.at[t, pl.ds(0, 31)], g_sem.at[0])
    sent = 3 + sum(1 if d in NEAR else 4 for d in range(1, 8))
    drain(r_c.at[pl.ds(0, sent)], c_send)

    @pl.when(mine)
    def _():
        drain(r_b.at[pl.ds(0, 31)], b_sem.at[0])

    @pl.when(jnp.logical_not(mine))
    def _():
        drain(r_b, b_sem.at[0])
        drain(s_c, c_send)

    for d in NEAR:

        @pl.when(zd[d] // 4 == t)
        def _():
            drain(r_c.at[pl.ds(0, 6)], c_send)

    drain(r_e.at[pl.ds(0, 31)], e_send)
    drain(r_m.at[pl.ds(0, 31)], m_sem.at[0])
    drain(r_y.at[pl.ds(0, 31)], y_sem.at[0])
    drain(r_h.at[pl.ds(0, 63)], h_sem.at[0])


def body(
    tokens, query_weight, key_weight, value_weight, gate_weight, decay_weight, decay_bias, states,
    head_gain, out_weight, norm1_gain, norm1_bias, up_weight, down_weight, norm2_gain, norm2_bias,
):
    flip = lambda w: w.transpose(1, 2, 0)
    flat = lambda w: flip(w).reshape(-1, D)
    line = lambda v: v.reshape(1, -1)
    vmem = pl.BlockSpec(memory_space=pltpu.VMEM)
    hbm = pl.BlockSpec(memory_space=pl.ANY)
    V = pltpu.VMEM
    dma = pltpu.SemaphoreType.DMA
    scratch = [
        V((64, 64), BF16), V((8, 128), F32), V((8, 256), F32),
        V((1, 64), F32), V((1, 64), F32), V((1, 64), F32), V((1, 64), F32),
        V((3, 8, 4, D), BF16),
        V((2, 224, D), BF16),
        V((2, 64, D), BF16),
        V((2, D, 256), BF16),
        V((2, 256, D), BF16),
        V((2, 8, 128, 256), F32),
        V((2, 16, 128), BF16), V((64, 16, 128), BF16),
        V((2, 128), F32), V((2, 32, 2, 128), F32),
        V((32, D), BF16),
        V((16, 2, 2, 256), BF16), V((32, 2, 256), BF16),
        V((16, 256), F32),
        V((16, 256), BF16), V((32, 16, 256), BF16),
        V((2, 256, 128), F32), V((32, D), BF16),
        V((32, 128), BF16), V((32, 32, 128), BF16),
        V((1, 128), F32), V((32, 1, 128), F32),
        V((32, 128), F32), V((32, 128), F32), V((2, 32, 256), F32),
        V((32, 32, 128), BF16), V((32, 32, 128), BF16),
        V((1, 128), F32), V((64, 1, 128), F32),
        V((32, 128), F32), V((32, 128), F32),
        V((128, 128), F32),
        dma((7,)), dma((9,)), dma((4,)), dma((4,)), dma, dma((16,)), dma, dma((8,)),
        dma((2,)), dma((2,)), dma((2,)), dma, dma((32,)), dma, dma((32,)),
    ] + [dma((2,))] * 4
    return pl.pallas_call(
        kernel,
        out_shape=(
            pltpu.VMEM((64, 64), BF16),
            pltpu.VMEM((2, 8, 128, 256), F32),
        ),
        in_specs=[hbm] * 16,
        out_specs=(vmem, vmem),
        scratch_shapes=scratch,
        compiler_params=pltpu.CompilerParams(
            collective_id=0, has_side_effects=True, vmem_limit_bytes=60 * 1024 * 1024
        ),
        name="layer_step",
    )(
        tokens, flip(query_weight), flip(key_weight), flip(decay_weight), flat(value_weight), flat(gate_weight),
        decay_bias, states, head_gain, out_weight.T, line(norm1_gain), line(norm1_bias), up_weight, down_weight,
        line(norm2_gain), line(norm2_bias),
    )


def solution(mesh):
    placed = (
        P("dp", ("kv", "tp")),
        P(None, "tp", "kv"),
        P(None, "tp", "kv"),
        P(None, "tp", "kv"),
        P(None, "tp", "kv"),
        P(None, "tp", "kv"),
        P("tp", None),
        P(("dp", "kv"), "tp", None, None),
        P("tp", None),
        P(None, ("kv", "tp")),
        P(("kv", "tp")),
        P(("kv", "tp")),
        P(None, ("kv", "tp")),
        P(("kv", "tp"), None),
        P(("kv", "tp")),
        P(("kv", "tp")),
    )
    return jax.shard_map(
        body,
        mesh=mesh,
        in_specs=placed,
        out_specs=(P("dp", ("kv", "tp")), P(("dp", "kv"), "tp", None, None)),
        check_vma=False,
    )
```
